256 devices in a mesh: ep: 16 (over y, x), tp: 16 (over z, core).
Axes of the slice: x: 4, y: 4, z: 8, core: 2. Of those that a mesh axis runs over, the one named last changes fastest.
Arguments:
- mixer_in: bfloat16 [65536, 2048], P(('ep', 'tp')), may hold values from -6 to 6
- pre_gain: float32 [2048], replicated, may hold values from 0.1 to 1.9
- glu_value: bfloat16 [2048, 1024], P(None, 'tp'), may hold values from -0.125 to 0.125
- glu_gate: bfloat16 [2048, 1024], P(None, 'tp'), may hold values from -0.125 to 0.125
- conv_kernel: float32 [31, 1024], replicated, may hold values from -1 to 1
- chan_gain: float32 [1024], replicated, may hold values from 0.1 to 1.9
- out_weight: bfloat16 [1024, 2048], P(None, 'tp'), may hold values from -0.1875 to 0.1875
- mix_gain: float32 [2048], replicated, may hold values from 0.1 to 1.9
- expert_in: bfloat16 [8192, 2048], P(('ep', 'tp')), may hold values from -6 to 6
- ffn_gain: float32 [2048], replicated, may hold values from 0.1 to 1.9
- routing: int32 [8192, 2], P(('ep', 'tp')), may hold values from 0 to 31, all different within a row; in each aligned block of 32 rows (0 to 31, 32 to 63, ...) at most 3 rows name the same one
- route_weight: float32 [8192, 2], P(('ep', 'tp')), may hold values from 0.1 to 1
- gate_proj: bfloat16 [32, 2048, 4096], P('ep', None, 'tp'), may hold values from -0.375 to 0.375
- up_proj: bfloat16 [32, 2048, 4096], P('ep', None, 'tp'), may hold values from -0.375 to 0.375
- down_proj: bfloat16 [32, 4096, 2048], P('ep', 'tp'), may hold values from -0.09375 to 0.09375
- expert_gain: float32 [2048], replicated, may hold values from 0.1 to 1.9
Outputs:
- mixed: bfloat16 [65536, 2048], P(('ep', 'tp'))
- routed: bfloat16 [8192, 2048], P(('ep', 'tp'))
The draws below stay inside these ranges and needn't reach their ends.
Inputs may be any that keep to these rules, and one draw needn't show every extreme that they name: `routing`: each row names 2 different experts; in each aligned block of 32 rows (the rows of one device) no expert is named more than 3 times.
All inputs are finite; a program needn't handle non-finite values.
Results may differ from the reference program's by a relative error of at most 0.02.
Values may be sent and summed in bfloat16 or wider, within the bound.
A program may use at most 128 MiB of HBM per device.

```python
import math
import jax
import jax.numpy as jnp
import numpy as np
from jax import lax

D = 2048
C = 1024
FF = 4096
KERNEL = 31
TOPK = 2
SLICE = 32
EXPERTS = 32
CAPS = 3
TOKENS1 = 65536
TOKENS2 = 8192
N_EP = 16
N_TP = 16


def levels(own_key, extent, cuts, low, top_value):
    gain, own = 1.0, jax.random.fold_in(own_key, 6)
    for dim, parts in cuts:
        steps = jnp.exp(jax.random.uniform(jax.random.fold_in(own, dim), (parts,), jnp.float32, low / len(cuts), top_value / len(cuts)))
        gain = gain * jnp.repeat(steps, extent[dim] // parts).reshape([-1 if axis == dim else 1 for axis in range(len(extent))])
    return gain


def assign_block(stream_key, own, number, rows, amount, top, limit, skew):
    sequence = jax.random.permutation(stream_key, amount)
    crowded, ordinary = portions_of(amount, rows * top, limit, skew, True), portions_of(amount, rows * top, limit, skew, False)
    places = jnp.arange(amount)

    def named(lengths, offset_by):
        used = int((lengths > 0).sum())
        fixed = max(1, used // 4)
        passed = fixed + (places - fixed + offset_by * (used - fixed)) % max(1, amount - fixed)
        return jnp.zeros((amount,), jnp.int32).at[sequence[jnp.where(places < fixed, places, passed)]].set(jnp.asarray(lengths, jnp.int32))

    lengths = jnp.where(number % 4 == 0, named(crowded, number // 4), named(ordinary, number - number // 4 - 1))
    mixed = jax.random.permutation(jax.random.fold_in(own, 3), amount)
    giver, taker = mixed[0:amount // 2 * 2:2], mixed[1:amount // 2 * 2:2]
    room = jnp.minimum(lengths[giver] - 1, limit - lengths[taker]) // 2
    room = jnp.where((giver == sequence[0]) | (taker == sequence[0]) | (lengths[taker] == 0), 0, jnp.maximum(room, 0))
    passed = jax.random.randint(jax.random.fold_in(own, 4), (amount // 2,), 0, 1 << 20) % (room + 1)
    lengths = lengths.at[giver].add(-passed).at[taker].add(passed)
    items = jnp.searchsorted(jnp.cumsum(lengths), jnp.arange(rows * top), side="right").astype(jnp.int32)
    table = items.reshape(top, rows).T
    table = table[jax.random.permutation(jax.random.fold_in(own, 1), rows)]
    offset_by = jax.random.randint(jax.random.fold_in(own, 2), (rows, 1), 0, top)
    return jnp.take_along_axis(table, (jnp.arange(top)[None, :] + offset_by) % top, axis=1)


def portions_of(count, total, limit, skew, full):
    portions = [(1 << 20) // math.isqrt(grade ** skew) + 1 for grade in range(1, count + 1)]
    largest = limit if full else min(limit, max(-(-total // count), total * portions[0] // sum(portions)))
    least = 1 if total - largest >= count - 1 else 0
    counts, surplus = [largest] + [least] * (count - 1), total - largest - least * (count - 1)
    while surplus > 0:
        candidates = [i for i in range(1, count) if counts[i] < largest] or [i for i in range(1, count) if counts[i] < limit]
        whole, remaining = sum([portions[i] for i in candidates]), surplus
        for i in candidates:
            extra = min(limit - counts[i], max(1, remaining * portions[i] // whole), surplus)
            counts[i] = counts[i] + extra
            surplus = surplus - extra
    return np.array(counts)


def normal_values(own_key, dims, deviation, bound, pieces=(), kind=jnp.bfloat16):
    gain = levels(own_key, dims, pieces, -0.22, 0.18) if pieces else 1.0
    array = jax.random.normal(own_key, dims, jnp.float32) * deviation * gain
    return jnp.minimum(jnp.maximum(array, -bound), bound).astype(kind)


def setup_inputs(seed: int = 0) -> dict:
    splits = jax.random.split(jax.random.key(seed), 17)
    mixer_in = normal_values(splits[0], (TOKENS1, D), 1.0, 6.0, ((0, 256),))
    pre_gain = jnp.clip(1.0 + 0.18 * jax.random.normal(splits[1], (D,), jnp.float32), 0.1, 1.9)
    glu_value = normal_values(splits[2], (D, C), D ** -0.5, 0.125, ((1, 16),))
    glu_gate = normal_values(splits[3], (D, C), D ** -0.5, 0.125, ((1, 16),))
    conv_kernel = normal_values(splits[4], (KERNEL, C), KERNEL ** -0.5, 1.0, (), jnp.float32)
    chan_gain = jnp.clip(1.0 + 0.18 * jax.random.normal(splits[5], (C,), jnp.float32), 0.1, 1.9)
    out_weight = normal_values(splits[6], (C, D), C ** -0.5, 0.1875, ((1, 16),))
    mix_gain = jnp.clip(1.0 + 0.18 * jax.random.normal(splits[7], (D,), jnp.float32), 0.1, 1.9)
    expert_in = normal_values(splits[8], (TOKENS2, D), 1.0, 6.0, ((0, 256),))
    ffn_gain = jnp.clip(1.0 + 0.18 * jax.random.normal(splits[9], (D,), jnp.float32), 0.1, 1.9)
    routing_keys = jax.random.split(jax.random.fold_in(splits[10], 1), TOKENS2 // SLICE)
    routing_turns = jax.random.permutation(jax.random.fold_in(splits[10], 3), TOKENS2 // SLICE)
    routing = jax.vmap(lambda own, number: assign_block(jax.random.fold_in(splits[10], 2), own, number, SLICE, EXPERTS, TOPK, CAPS, 2))(routing_keys, routing_turns).reshape((TOKENS2, TOPK))
    route_weight = jnp.clip(0.1 + 0.9 * jax.random.uniform(splits[11], (TOKENS2, TOPK), jnp.float32) ** levels(splits[11], (TOKENS2, TOPK), ((0, 256),), -0.2, 0.2), 0.1, 1.0)
    gate_proj = normal_values(splits[12], (EXPERTS, D, FF), (D // 9) ** -0.5, 0.375, ((0, 16), (2, 16)))
    up_proj = normal_values(splits[13], (EXPERTS, D, FF), (D // 9) ** -0.5, 0.375, ((0, 16), (2, 16)))
    down_proj = normal_values(splits[14], (EXPERTS, FF, D), FF ** -0.5, 0.09375, ((0, 16), (1, 16)))
    expert_gain = jnp.clip(1.0 + 0.18 * jax.random.normal(splits[15], (D,), jnp.float32), 0.1, 1.9)
    return dict(mixer_in=mixer_in, pre_gain=pre_gain, glu_value=glu_value, glu_gate=glu_gate, conv_kernel=conv_kernel, chan_gain=chan_gain, out_weight=out_weight, mix_gain=mix_gain, expert_in=expert_in, ffn_gain=ffn_gain, routing=routing, route_weight=route_weight, gate_proj=gate_proj, up_proj=up_proj, down_proj=down_proj, expert_gain=expert_gain)


RMS_EPSILON = 1e-06
LAYER_EPSILON = 1e-05
CLAMP_LIMIT = 7.0
SWISH_ALPHA = 1.702

def rms_scale(values, gain_row):
    values = values.astype(jnp.float32)
    return values * lax.rsqrt(lax.optimization_barrier(jnp.mean(values * values, axis=-1, keepdims=True)) + RMS_EPSILON) * gain_row

def conv_mixer(mixer_in, pre_gain, glu_value, glu_gate, conv_kernel, chan_gain, out_weight, mix_gain):
    normed = rms_scale(mixer_in, pre_gain).astype(jnp.bfloat16)
    value_pre = jnp.dot(normed, glu_value, preferred_element_type=jnp.float32)
    gate_pre = jnp.dot(normed, glu_gate, preferred_element_type=jnp.float32)
    gated_rows = (value_pre * jax.nn.sigmoid(gate_pre)).astype(jnp.bfloat16)
    length = gated_rows.shape[0]
    padded = jnp.pad(gated_rows.astype(jnp.float32), ((KERNEL - 1, 0), (0, 0)))
    conv_sum = jnp.zeros((length, gated_rows.shape[1]), jnp.float32)
    for offset in range(KERNEL):
        conv_sum = conv_sum + conv_kernel[offset] * padded[offset:offset + length]
    row_mean = lax.optimization_barrier(jnp.mean(conv_sum, axis=-1, keepdims=True))
    centred = conv_sum - row_mean
    row_var = lax.optimization_barrier(jnp.mean(centred * centred, axis=-1, keepdims=True))
    activated = jax.nn.silu(centred * lax.rsqrt(row_var + LAYER_EPSILON) * chan_gain).astype(jnp.bfloat16)
    projected = jnp.dot(activated, out_weight, preferred_element_type=jnp.float32)
    return rms_scale(projected, mix_gain).astype(jnp.bfloat16)

def expert_layer(expert_in, ffn_gain, routing, route_weight, gate_proj, up_proj, down_proj, expert_gain):
    normed = rms_scale(expert_in, ffn_gain).astype(jnp.bfloat16)
    flat_route = routing.reshape(-1)
    flat_weight = route_weight.reshape(-1)
    capacity = N_EP * N_TP * CAPS
    hidden = gate_proj.shape[2] // N_TP

    def one_expert(running, expert):
        matches = flat_route == expert
        entry_index = jnp.nonzero(matches, size=capacity, fill_value=0)[0].astype(jnp.int32)
        live_count = jnp.sum(matches.astype(jnp.int32))
        live_slot = jnp.arange(capacity, dtype=jnp.int32) < live_count
        token_index = (entry_index // TOPK).astype(jnp.int32)
        row_block = normed[token_index]
        gate_pre = jnp.dot(row_block, gate_proj[expert], preferred_element_type=jnp.float32)
        up_pre = jnp.dot(row_block, up_proj[expert], preferred_element_type=jnp.float32)
        gate_pre = jnp.minimum(gate_pre, CLAMP_LIMIT)
        up_pre = jnp.clip(up_pre, -CLAMP_LIMIT, CLAMP_LIMIT)
        hidden_act = ((up_pre + 1.0) * gate_pre * jax.nn.sigmoid(SWISH_ALPHA * gate_pre)).astype(jnp.bfloat16)
        blocks = hidden_act.reshape(capacity, N_TP, hidden).astype(jnp.float32)
        down_block = down_proj[expert].reshape(N_TP, hidden, -1).astype(jnp.float32)
        partial_value = jnp.einsum('rnf,nfd->nrd', blocks, down_block).astype(jnp.bfloat16)
        expert_out = lax.optimization_barrier(jnp.sum(partial_value.astype(jnp.float32), axis=0)).astype(jnp.bfloat16)
        slot_weight = jnp.where(live_slot, flat_weight[entry_index], 0.0)
        running = running.at[token_index].add(slot_weight[:, None] * expert_out.astype(jnp.float32))
        return (running, None)
    start_sum = jnp.zeros(expert_in.shape, jnp.float32)
    combined, unused = lax.scan(one_expert, start_sum, jnp.arange(EXPERTS, dtype=jnp.int32))
    return rms_scale(combined, expert_gain).astype(jnp.bfloat16)

def reference(mixer_in, pre_gain, glu_value, glu_gate, conv_kernel, chan_gain, out_weight, mix_gain, expert_in, ffn_gain, routing, route_weight, gate_proj, up_proj, down_proj, expert_gain):
    mixed = conv_mixer(mixer_in, pre_gain, glu_value, glu_gate, conv_kernel, chan_gain, out_weight, mix_gain)
    routed = expert_layer(expert_in, ffn_gain, routing, route_weight, gate_proj, up_proj, down_proj, expert_gain)
    return (mixed, routed)
```

```python
import functools

import jax
import jax.numpy as jnp
from jax import lax
from jax.experimental import pallas as pl
from jax.experimental.pallas import tpu as pltpu
from jax.sharding import PartitionSpec as P

RMS_EPSILON = 1e-06
LAYER_EPSILON = 1e-05
CLAMP_LIMIT = 7.0
SWISH_ALPHA = 1.702
CAPS = 3
MESH = pl.DeviceIdType.MESH
F32 = jnp.float32
BF16 = jnp.bfloat16


def iota(shape, dim):
    return lax.broadcasted_iota(jnp.int32, shape, dim)


def mm(a, b):
    return jnp.dot(a, b, preferred_element_type=F32)


def rms_scale(values, gain_row):
    values = values.astype(F32)
    return (
        values
        * lax.rsqrt(jnp.mean(values * values, axis=-1, keepdims=True) + RMS_EPSILON)
        * gain_row
    )


def expert_kernel(
    n_ep,
    n_z,
    x_ref,
    fgain_ref,
    route_ref,
    rw_ref,
    egain_ref,
    gate_hbm,
    up_hbm,
    down_hbm,
    out_ref,
    gate_v,
    up_v,
    down_v,
    slab,
    arrived,
    rows,
    parts,
    mate,
    ring_in,
    back_slab,
    back,
    w_sem,
    a_send,
    a_recv,
    g_send,
    g_recv,
    m_send,
    m_recv,
    q_send,
    q_recv,
    s_send,
    s_recv,
    b_send,
    b_recv,
):
    half_z = n_z // 2
    tokens, width = x_ref.shape
    half = width // 2
    cap = n_ep * CAPS
    slots = n_ep * 16
    ep, tp = lax.axis_index("ep"), lax.axis_index("tp")
    z, core = tp // 2, tp % 2
    mate_tp = 2 * z + 1 - core
    next_tp = 2 * ((z + 1) % n_z) + core
    prev_tp = 2 * ((z + n_z - 1) % n_z) + core
    toward = {1: next_tp, -1: prev_tp}
    side = {1: 0, -1: 1}

    def pos(d):
        d = (d + half_z - 1) % n_z - (half_z - 1)
        return 2 * d - 1 if d > 0 else -2 * d

    def place(d):
        return n_z - 1 if d in (half_z, -half_z) else pos(d)

    def hops(way, e):
        return half_z if (way == 1) == (e == 0) else half_z - 1

    loads = [
        pltpu.make_async_copy(src, dst, w_sem.at[i])
        for i, (src, dst) in enumerate(
            ((gate_hbm, gate_v), (up_hbm, up_v), (down_hbm, down_v))
        )
    ]
    for load in loads:
        load.start()

    barrier = pltpu.get_barrier_semaphore()

    def greet(i, carry):
        pl.semaphore_signal(
            barrier, inc=1, device_id=((ep + i) % n_ep, tp), device_id_type=MESH
        )
        return carry

    lax.fori_loop(1, n_ep, greet, 0)
    for other in (mate_tp, next_tp, prev_tp):
        pl.semaphore_signal(
            barrier, inc=1, device_id=(ep, other), device_id_type=MESH
        )

    experts = 2 * n_ep
    chosen = [route_ref[:, k : k + 1] for k in range(2)]
    named = [
        (c == iota((tokens, experts), 1)).astype(F32) for c in chosen
    ]
    earlier = (iota((tokens, tokens), 1) < iota((tokens, tokens), 0)).astype(F32)
    before = mm(earlier.astype(BF16), (named[0] + named[1]).astype(BF16))
    spot = [
        (c // 2) * 16
        + (c % 2) * CAPS
        + jnp.sum(before * n, axis=1, keepdims=True).astype(jnp.int32)
        for c, n in zip(chosen, named)
    ]
    eye = iota((tokens, tokens), 0) == iota((tokens, tokens), 1)
    spot_row = [
        jnp.sum(jnp.where(eye, s.astype(F32), 0.0), axis=0, keepdims=True).astype(
            jnp.int32
        )
        for s in spot
    ]
    normed = rms_scale(x_ref[...], fgain_ref[...]).astype(BF16)
    picked = jnp.zeros((slots, half), F32)
    for h in range(2):
        at = iota((slots, tokens), 0) - 8 * h
        hit = jnp.logical_or(at == spot_row[0], at == spot_row[1])
        picked = picked + mm(
            jnp.where(hit, 1.0, 0.0).astype(BF16), normed[:, h * half : (h + 1) * half]
        )
    slab[...] = picked.astype(BF16).reshape(n_ep, 16, half)
    pl.semaphore_wait(barrier, n_ep - 1 + 3)

    def exchange(src, dst, send, recv):
        def copy(i):
            peer = (ep + i) % n_ep
            return pltpu.make_async_remote_copy(
                src_ref=src.at[peer],
                dst_ref=dst.at[ep],
                send_sem=send.at[i],
                recv_sem=recv.at[i],
                device_id=(peer, tp),
                device_id_type=MESH,
            )

        return copy

    def run(fn, low, high):
        def body(i, carry):
            fn(i)
            return carry

        lax.fori_loop(low, high, body, 0)

    out_copy = exchange(slab, arrived, a_send, a_recv)
    run(lambda i: out_copy(i).start(), 1, n_ep)
    arrived[ep] = slab[ep]
    run(lambda i: out_copy(i).wait_recv(), 1, n_ep)

    def to_rows(e, h, shape, row_dim, slot_dim):
        row, slot = iota(shape, row_dim), iota(shape, slot_dim)
        inner = slot % 8 - CAPS * e
        hit = (row == (slot // 16) * CAPS + inner) & ((slot // 8) % 2 == h)
        hit = hit & (inner >= 0) & (inner < CAPS)
        return jnp.where(hit, 1.0, 0.0).astype(BF16)

    def ring(way, e, k):
        return pltpu.make_async_remote_copy(
            src_ref=rows.at[e, place(-way * (k - 1)), 0],
            dst_ref=rows.at[e, place(-way * k), 0],
            send_sem=g_send.at[side[way], e, k - 1],
            recv_sem=g_recv.at[side[way], e, k - 1],
            device_id=(ep, toward[way]),
            device_id_type=MESH,
        )

    def to_mate(e, p):
        return pltpu.make_async_remote_copy(
            src_ref=rows.at[e, p, 0],
            dst_ref=rows.at[e, p, 1],
            send_sem=m_send.at[e, p],
            recv_sem=m_recv.at[e, p],
            device_id=(ep, mate_tp),
            device_id_type=MESH,
        )

    def part_to_mate(e, p):
        return pltpu.make_async_remote_copy(
            src_ref=parts.at[e, p, 1],
            dst_ref=mate.at[e, p],
            send_sem=q_send.at[e, p],
            recv_sem=q_recv.at[e, p],
            device_id=(ep, mate_tp),
            device_id_type=MESH,
        )

    def ring_sum(way, e, k):
        return pltpu.make_async_remote_copy(
            src_ref=parts.at[e, place(way * k), 0],
            dst_ref=ring_in.at[side[way], e, k - 1],
            send_sem=s_send.at[side[way], e, k - 1],
            recv_sem=s_recv.at[side[way], e, k - 1],
            device_id=(ep, toward[way]),
            device_id_type=MESH,
        )

    block = arrived[...].reshape(slots, half)
    for e in range(2):
        for h in range(2):
            rows[e, 0, 0, :, h * half : (h + 1) * half] = mm(
                to_rows(e, h, (cap, slots), 0, 1), block
            ).astype(BF16)
        for way in (1, -1):
            ring(way, e, 1).start()
        to_mate(e, 0).start()
    for load in loads:
        load.wait()

    def ffn(low, high):
        for e in range(2):
            for p in range(low, high):
                to_mate(e, p).wait_recv()
        count = (high - low) * 2 * cap

        def one(e, carry):
            block = rows[e, low:high].reshape(count, width)
            gate = jnp.minimum(mm(block, gate_v[e]), CLAMP_LIMIT)
            up = jnp.clip(mm(block, up_v[e]), -CLAMP_LIMIT, CLAMP_LIMIT)
            hidden = ((up + 1.0) * gate * jax.nn.sigmoid(SWISH_ALPHA * gate)).astype(
                BF16
            )
            parts[e, low:high] = (
                mm(hidden, down_v[e])
                .astype(BF16)
                .reshape(high - low, 2, cap, width)
            )
            return carry

        lax.fori_loop(0, 2, one, 0)
        for e in range(2):
            for p in range(low, high):
                part_to_mate(e, p).start()

    def chip_sum(low, high):
        for e in range(2):
            for p in range(low, high):
                part_to_mate(e, p).wait_recv()
                parts[e, p, 0] = (
                    parts[e, p, 0].astype(F32) + mate[e, p].astype(F32)
                ).astype(BF16)

    ffn(0, 1)
    for k in range(1, half_z + 1):
        for e in range(2):
            for way in (1, -1):
                if k <= hops(way, e):
                    ring(way, e, k).wait_recv()
                    if k < hops(way, e):
                        ring(way, e, k + 1).start()
                    to_mate(e, place(-way * k)).start()
        if k < half_z:
            ffn(2 * k - 1, 2 * k + 1)
            if k == half_z - 1:
                chip_sum(0, 2 * k + 1)
                for e in range(2):
                    for way in (1, -1):
                        if hops(way, e) == k:
                            ring_sum(way, e, k).start()
        else:
            ffn(n_z - 1, n_z)
            chip_sum(n_z - 1, n_z)

    for k in range(half_z, 0, -1):
        for e in range(2):
            for way in (1, -1):
                if k < hops(way, e):
                    ring_sum(way, e, k + 1).wait_recv()
                    p = place(way * k)
                    parts[e, p, 0] = (
                        parts[e, p, 0].astype(F32)
                        + ring_in[side[way], e, k].astype(F32)
                    ).astype(BF16)
                    ring_sum(way, e, k).start()
                elif k == half_z and hops(way, e) == k:
                    ring_sum(way, e, k).start()
    done = []
    for e in range(2):
        for way in (1, -1):
            ring_sum(way, e, 1).wait_recv()
        done.append(
            (
                parts[e, 0, 0].astype(F32)
                + ring_in[0, e, 0].astype(F32)
                + ring_in[1, e, 0].astype(F32)
            ).astype(BF16)
        )

    back_rows = jnp.zeros((slots, half), F32)
    for e in range(2):
        for h in range(2):
            back_rows = back_rows + mm(
                to_rows(e, h, (slots, cap), 1, 0), done[e][:, h * half : (h + 1) * half]
            )
    back_slab[...] = back_rows.astype(BF16).reshape(n_ep, 16, half)
    back_copy = exchange(back_slab, back, b_send, b_recv)
    run(lambda i: back_copy(i).start(), 1, n_ep)
    back[ep] = back_slab[ep]
    mixes = []
    for h in range(2):
        at = iota((tokens, slots), 1) - 8 * h
        share = jnp.zeros((tokens, slots), F32)
        for k in range(2):
            share = share + jnp.where(at == spot[k], rw_ref[:, k : k + 1], 0.0)
        high = share.astype(BF16)
        mixes.append((high, (share - high.astype(F32)).astype(BF16)))
    run(lambda i: back_copy(i).wait_recv(), 1, n_ep)
    results = back[...].reshape(slots, half)
    combined = [mm(high, results) + mm(low, results) for high, low in mixes]
    square = sum(jnp.sum(c * c, axis=1, keepdims=True) for c in combined)
    scale = lax.rsqrt(square / width + RMS_EPSILON)
    for h in range(2):
        cols = slice(h * half, (h + 1) * half)
        out_ref[:, cols] = (combined[h] * scale * egain_ref[:, cols]).astype(BF16)

    run(lambda i: out_copy(i).wait_send(), 1, n_ep)
    run(lambda i: back_copy(i).wait_send(), 1, n_ep)
    for e in range(2):
        for way in (1, -1):
            for k in range(1, hops(way, e) + 1):
                ring(way, e, k).wait_send()
                ring_sum(way, e, k).wait_send()
        for p in range(n_z):
            to_mate(e, p).wait_send()
            part_to_mate(e, p).wait_send()


def experts_path(
    expert_in, ffn_gain, routing, route_weight, gate_proj, up_proj, down_proj, expert_gain
):
    n_ep, n_z = lax.axis_size("ep"), lax.axis_size("tp") // 2
    half_z = n_z // 2
    tokens, width = expert_in.shape
    half, cap, hid = width // 2, n_ep * CAPS, gate_proj.shape[2]
    dma = pltpu.SemaphoreType.DMA
    vmem = pl.BlockSpec(memory_space=pltpu.VMEM)
    hbm = pl.BlockSpec(memory_space=pl.ANY)
    return pl.pallas_call(
        functools.partial(expert_kernel, n_ep, n_z),
        out_shape=jax.ShapeDtypeStruct((tokens, width), BF16),
        in_specs=[vmem] * 5 + [hbm] * 3,
        out_specs=vmem,
        scratch_shapes=[
            pltpu.VMEM((2, width, hid), BF16),
            pltpu.VMEM((2, width, hid), BF16),
            pltpu.VMEM((2, hid, width), BF16),
            pltpu.VMEM((n_ep, 16, half), BF16),
            pltpu.VMEM((n_ep, 16, half), BF16),
            pltpu.VMEM((2, n_z, 2, cap, width), BF16),
            pltpu.VMEM((2, n_z, 2, cap, width), BF16),
            pltpu.VMEM((2, n_z, cap, width), BF16),
            pltpu.VMEM((2, 2, half_z, cap, width), BF16),
            pltpu.VMEM((n_ep, 16, half), BF16),
            pltpu.VMEM((n_ep, 16, half), BF16),
            dma((3,)),
            dma((n_ep,)),
            dma((n_ep,)),
            dma((2, 2, half_z)),
            dma((2, 2, half_z)),
            dma((2, n_z)),
            dma((2, n_z)),
            dma((2, n_z)),
            dma((2, n_z)),
            dma((2, 2, half_z)),
            dma((2, 2, half_z)),
            dma((n_ep,)),
            dma((n_ep,)),
        ],
        compiler_params=pltpu.CompilerParams(
            collective_id=0, has_side_effects=True, vmem_limit_bytes=60 * 1024 * 1024
        ),
        cost_estimate=pl.CostEstimate(
            flops=80_000_000_000, bytes_accessed=16_000_000, transcendentals=0
        ),
        name="experts",
    )(
        expert_in,
        ffn_gain.reshape(1, -1),
        routing,
        route_weight,
        expert_gain.reshape(1, -1),
        gate_proj,
        up_proj,
        down_proj,
    )


def passed_along(value, axis, steps):
    count = lax.axis_size(axis)
    initial, last = (max(0, -steps), min(count, count - steps))
    return lax.ppermute(value, axis, [(source, source + steps) for source in range(initial, last)])


def on_device(
    mixer_in,
    pre_gain,
    glu_value,
    glu_gate,
    conv_kernel,
    chan_gain,
    out_weight,
    mix_gain,
    expert_in,
    ffn_gain,
    routing,
    route_weight,
    gate_proj,
    up_proj,
    down_proj,
    expert_gain,
):
    n_ep, n_tp, ep = lax.axis_size("ep"), lax.axis_size("tp"), lax.axis_index("ep")
    width, cols = glu_value.shape
    channels = cols * n_tp
    both = jnp.concatenate([glu_value, glu_gate], axis=1)
    rows_v, rows_o = width // n_ep, channels // n_ep
    piece = jnp.concatenate(
        [
            lax.dynamic_slice_in_dim(both, ep * rows_v, rows_v, 0),
            lax.dynamic_slice_in_dim(out_weight, ep * rows_o, rows_o, 0),
        ],
        axis=0,
    )
    full = lax.all_gather(piece, ("ep", "tp"), axis=0, tiled=False)
    full = full.reshape(n_ep, n_tp, rows_v + rows_o, 2 * cols)
    routed = experts_path(
        expert_in, ffn_gain, routing, route_weight, gate_proj, up_proj, down_proj, expert_gain
    )
    glu_full = full[:, :, :rows_v].transpose(0, 2, 1, 3).reshape(width, n_tp * 2 * cols)
    out_full = full[:, :, rows_v:].transpose(0, 2, 1, 3).reshape(channels, width)
    normed_mix = rms_scale(mixer_in, pre_gain).astype(BF16)
    pre = mm(normed_mix, glu_full).reshape(-1, n_tp, 2, cols)
    gated = pre[:, :, 0] * jax.nn.sigmoid(pre[:, :, 1])
    gated_rows = gated.reshape(-1, channels).astype(BF16)
    kernel_width = conv_kernel.shape[0]
    length = gated_rows.shape[0]
    rim_rows = passed_along(gated_rows[length - (kernel_width - 1) :], ("ep", "tp"), 1)
    padded = jnp.concatenate([rim_rows, gated_rows], axis=0).astype(F32)
    conv_sum = jnp.zeros((length, channels), F32)
    for offset in range(kernel_width):
        conv_sum = conv_sum + conv_kernel[offset] * padded[offset : offset + length]
    row_mean = jnp.mean(conv_sum, axis=-1, keepdims=True)
    centred = conv_sum - row_mean
    row_var = jnp.mean(centred * centred, axis=-1, keepdims=True)
    activated = jax.nn.silu(centred * lax.rsqrt(row_var + LAYER_EPSILON) * chan_gain).astype(BF16)
    projected = mm(activated, out_full)
    mixed = rms_scale(projected, mix_gain).astype(BF16)
    return (mixed, routed)


def solution(mesh):
    in_specs = (
        P(("ep", "tp"), None),
        P(),
        P(None, "tp"),
        P(None, "tp"),
        P(),
        P(),
        P(None, "tp"),
        P(),
        P(("ep", "tp"), None),
        P(),
        P(("ep", "tp"), None),
        P(("ep", "tp"), None),
        P("ep", None, "tp"),
        P("ep", None, "tp"),
        P("ep", "tp", None),
        P(),
    )
    out_specs = (P(("ep", "tp"), None), P(("ep", "tp"), None))
    return jax.shard_map(
        on_device, mesh=mesh, in_specs=in_specs, out_specs=out_specs, check_vma=False
    )
```

```python
import functools

import jax
import jax.numpy as jnp
from jax import lax
from jax.experimental import pallas as pl
from jax.experimental.pallas import tpu as pltpu
from jax.sharding import PartitionSpec as P

RMS_EPSILON = 1e-06
LAYER_EPSILON = 1e-05
CLAMP_LIMIT = 7.0
SWISH_ALPHA = 1.702
CAPS = 3
MESH = pl.DeviceIdType.MESH
F32 = jnp.float32
BF16 = jnp.bfloat16


def iota(shape, dim):
    return lax.broadcasted_iota(jnp.int32, shape, dim)


def mm(a, b):
    return jnp.dot(a, b, preferred_element_type=F32)


def rms_scale(values, gain_row):
    values = values.astype(F32)
    return (
        values
        * lax.rsqrt(jnp.mean(values * values, axis=-1, keepdims=True) + RMS_EPSILON)
        * gain_row
    )


def both_kernel(
    n_ep,
    n_z,
    x_ref,
    fgain_ref,
    route_ref,
    rw_ref,
    egain_ref,
    pgain_ref,
    taps_ref,
    cgain_ref,
    mgain_ref,
    gate_hbm,
    up_hbm,
    down_hbm,
    mix_hbm,
    value_hbm,
    glu_hbm,
    ow_hbm,
    out_ref,
    mixed_hbm,
    gate_v,
    up_v,
    down_v,
    mix_v,
    loc_vg,
    loc_o,
    slab,
    arrived,
    rows,
    parts,
    mate,
    ring_in,
    back_slab,
    back,
    vg_all,
    o_all,
    normed_v,
    ext,
    tail_rows,
    rim,
    conv_v,
    act_v,
    proj_v,
    mixed_v,
    w_sem,
    a_send,
    a_recv,
    g_send,
    g_recv,
    m_send,
    m_recv,
    q_send,
    q_recv,
    s_send,
    s_recv,
    b_send,
    b_recv,
    c_send,
    c_recv,
    p_send,
    p_recv,
    t_send,
    t_recv,
    h_sem,
    o_sem,
):
    half_z = n_z // 2
    n_s = 4
    tokens, width = x_ref.shape
    half = width // 2
    cap = n_ep * CAPS
    slots = n_ep * 16
    length = mix_v.shape[0]
    unit = width // n_ep
    o_unit = loc_o.shape[1] // n_ep
    ep, tp = lax.axis_index("ep"), lax.axis_index("tp")
    z, core = tp // 2, tp % 2
    mate_tp = 2 * z + 1 - core
    next_tp = 2 * ((z + 1) % n_z) + core
    prev_tp = 2 * ((z + n_z - 1) % n_z) + core
    toward = {1: next_tp, -1: prev_tp}
    side = {1: 0, -1: 1}
    major = (ep // n_s, ep % n_s)
    minor = (ep % n_s, ep // n_s)
    after = (tp + 1) // (2 * n_z)
    line_next = ((ep + after) % n_ep, (tp + 1) % (2 * n_z))
    behind = (2 * n_z - tp) // (2 * n_z)
    line_prev = ((ep + n_ep - behind) % n_ep, (tp + 2 * n_z - 1) % (2 * n_z))

    def pos(d):
        return 2 * d - 1 if d > 0 else -2 * d

    def place(d):
        return n_z - 1 if d in (half_z, -half_z) else pos(d)

    def hops(way, e):
        return half_z if (way == 1) == (e == 0) else half_z - 1

    def send(src, dst, send_sem, recv_sem, device):
        return pltpu.make_async_remote_copy(
            src_ref=src,
            dst_ref=dst,
            send_sem=send_sem,
            recv_sem=recv_sem,
            device_id=device,
            device_id_type=MESH,
        )

    def run(fn, low, high):
        def body(i, carry):
            fn(i)
            return carry

        lax.fori_loop(low, high, body, 0)

    def lanes(i, n):
        return pl.ds(pl.multiple_of(i * n, n), n)

    loads = [
        pltpu.make_async_copy(src, dst, w_sem.at[i])
        for i, (src, dst) in enumerate(
            (
                (value_hbm, loc_vg.at[0]),
                (glu_hbm, loc_vg.at[1]),
                (ow_hbm, loc_o),
                (gate_hbm, gate_v),
                (up_hbm, up_v),
                (down_hbm, down_v),
                (mix_hbm, mix_v),
            )
        )
    ]
    for load in loads:
        load.start()

    barrier = pltpu.get_barrier_semaphore()

    def greet(device):
        pl.semaphore_signal(barrier, inc=1, device_id=device, device_id_type=MESH)

    run(lambda i: greet(((ep + i) % n_ep, tp)), 1, n_ep)
    run(lambda i: greet((ep, 2 * ((z + i) % n_z) + core)), 1, n_z)
    for device in ((ep, mate_tp), line_next, line_prev):
        greet(device)

    experts = 2 * n_ep
    eye = iota((tokens, tokens), 0) == iota((tokens, tokens), 1)

    def upright(row):
        return jnp.sum(jnp.where(eye, row, 0.0), axis=1, keepdims=True)

    chosen = [route_ref[k : k + 1, :] for k in range(2)]
    named = [(c == iota((experts, tokens), 0)).astype(F32) for c in chosen]
    earlier = (iota((tokens, tokens), 0) < iota((tokens, tokens), 1)).astype(F32)
    before = mm((named[0] + named[1]).astype(BF16), earlier.astype(BF16))
    spot_row = [
        (c // 2) * 16
        + (c % 2) * CAPS
        + jnp.sum(before * n, axis=0, keepdims=True).astype(jnp.int32)
        for c, n in zip(chosen, named)
    ]
    normed = rms_scale(x_ref[...], fgain_ref[...]).astype(BF16)
    picked = jnp.zeros((slots, half), F32)
    for h in range(2):
        at = iota((slots, tokens), 0) - 8 * h
        hit = jnp.logical_or(at == spot_row[0], at == spot_row[1])
        picked = picked + mm(
            jnp.where(hit, 1.0, 0.0).astype(BF16), normed[:, h * half : (h + 1) * half]
        )
    slab[...] = picked.astype(BF16).reshape(n_ep, 16, half)
    pl.semaphore_wait(barrier, n_ep - 1 + n_z - 1 + 3)

    def exchange(src, dst, send_sem, recv_sem):
        def copy(i):
            peer = (ep + i) % n_ep
            return send(
                src.at[peer], dst.at[ep], send_sem.at[i], recv_sem.at[i], (peer, tp)
            )

        return copy

    out_copy = exchange(slab, arrived, a_send, a_recv)
    run(lambda i: out_copy(i).start(), 1, n_ep)

    piece = [major[i] * n_s + minor[i] for i in range(2)]

    def vg_at(i, zs, who, at, count):
        return vg_all.at[i, zs, who, :, pl.ds(pl.multiple_of(at * unit, unit), count * unit)]

    def o_at(i, zs, who, at, count):
        return o_all.at[
            i, zs, pl.ds(pl.multiple_of(at * o_unit, o_unit), count * o_unit), lanes(who, 128)
        ]

    def column_copies(dz):
        device = (ep, 2 * ((z + dz) % n_z) + core)
        copies = []
        for i in range(2):
            copies.append(
                send(
                    loc_vg.at[i, :, lanes(piece[i], unit)],
                    vg_at(i, z, core, piece[i], 1),
                    c_send.at[dz, 2 * i],
                    c_recv.at[dz, 2 * i],
                    device,
                )
            )
            copies.append(
                send(
                    loc_o.at[i, lanes(piece[i], o_unit), :],
                    o_at(i, z, core, piece[i], 1),
                    c_send.at[dz, 2 * i + 1],
                    c_recv.at[dz, 2 * i + 1],
                    device,
                )
            )
        return copies

    own_copies = []
    for i in range(2):
        own_copies.append(
            pltpu.make_async_copy(
                loc_vg.at[i, :, lanes(piece[i], unit)],
                vg_at(i, z, core, piece[i], 1),
                h_sem.at[2 * i],
            )
        )
        own_copies.append(
            pltpu.make_async_copy(
                loc_o.at[i, lanes(piece[i], o_unit), :],
                o_at(i, z, core, piece[i], 1),
                h_sem.at[2 * i + 1],
            )
        )
    for load in loads[:3]:
        load.wait()

    def column_start(dz):
        for copy in column_copies(dz):
            copy.start()

    run(column_start, 1, n_z)
    for copy in own_copies:
        copy.start()
    arrived[ep] = slab[ep]

    def plane(i, phase, way, step):
        a, b = major[i], minor[i]
        zs = pl.ds(0, n_z) if step == 0 else pl.ds(0 if way == 1 else half_z, half_z)
        if phase == 0:
            source = (b + n_s - way * step) % n_s
            at, count = a * n_s + source, 1
            there = (a, (b + n_s + way) % n_s)
        else:
            source = (a + n_s - way * step) % n_s
            at, count = source * n_s, n_s
            there = ((a + n_s + way) % n_s, b)
        device = (there[0] * n_s + there[1] if i == 0 else there[1] * n_s + there[0], tp)
        mark = 2 * step + side[way]
        vg, o = vg_at(i, zs, core, at, count), o_at(i, zs, core, at, count)
        return [
            send(
                ref,
                ref,
                p_send.at[i, phase, 2 * mark + n],
                p_recv.at[i, phase, 2 * mark + n],
                device,
            )
            for n, ref in enumerate((vg, o))
        ]

    def plane_mate(i, turn):
        shift = (0, n_s - 1, 1, 2)[turn]
        at = ((major[i] + shift) % n_s) * n_s
        zs = pl.ds(0, n_z)
        return [
            send(ref, ref, t_send.at[i, turn, n], t_recv.at[i, turn, n], (ep, mate_tp))
            for n, ref in enumerate((vg_at(i, zs, core, at, n_s), o_at(i, zs, core, at, n_s)))
        ]

    def start(copies):
        for copy in copies:
            copy.start()

    def landed(copies):
        for copy in copies:
            copy.wait_recv()

    def left(copies):
        for copy in copies:
            copy.wait_send()

    run(lambda i: out_copy(i).wait_recv(), 1, n_ep)

    def to_rows(e, h, shape, row_dim, slot_dim):
        row, slot = iota(shape, row_dim), iota(shape, slot_dim)
        inner = slot % 8 - CAPS * e
        hit = (row == (slot // 16) * CAPS + inner) & ((slot // 8) % 2 == h)
        hit = hit & (inner >= 0) & (inner < CAPS)
        return jnp.where(hit, 1.0, 0.0).astype(BF16)

    def ring(way, e, k):
        return send(
            rows.at[e, place(-way * (k - 1)), 0],
            rows.at[e, place(-way * k), 0],
            g_send.at[side[way], e, k - 1],
            g_recv.at[side[way], e, k - 1],
            (ep, toward[way]),
        )

    def to_mate(e, p):
        return send(
            rows.at[e, p, 0], rows.at[e, p, 1], m_send.at[e, p], m_recv.at[e, p], (ep, mate_tp)
        )

    def part_to_mate(e, p):
        return send(
            parts.at[e, p, 1], mate.at[e, p], q_send.at[e, p], q_recv.at[e, p], (ep, mate_tp)
        )

    def ring_sum(way, e, k):
        return send(
            parts.at[e, place(way * k), 0],
            ring_in.at[side[way], e, k - 1],
            s_send.at[side[way], e, k - 1],
            s_recv.at[side[way], e, k - 1],
            (ep, toward[way]),
        )

    block = arrived[...].reshape(slots, half)
    for e in range(2):
        for h in range(2):
            rows[e, 0, 0, :, h * half : (h + 1) * half] = mm(
                to_rows(e, h, (cap, slots), 0, 1), block
            ).astype(BF16)
        for way in (1, -1):
            if hops(way, e) > 0:
                ring(way, e, 1).start()
        to_mate(e, 0).start()

    def column_landed(dz):
        landed(column_copies(dz))

    run(column_landed, 1, n_z)
    for copy in own_copies:
        copy.wait()
    for i in range(2):
        for way in (1, -1):
            start(plane(i, 0, way, 0))
    for load in loads[3:]:
        load.wait()

    def ffn(low, high):
        for e in range(2):
            for p in range(low, high):
                to_mate(e, p).wait_recv()
        count = (high - low) * 2 * cap

        def one(e):
            block = rows[e, low:high].reshape(count, width)
            gate = jnp.minimum(mm(block, gate_v[e]), CLAMP_LIMIT)
            up = jnp.clip(mm(block, up_v[e]), -CLAMP_LIMIT, CLAMP_LIMIT)
            hidden = ((up + 1.0) * gate * jax.nn.sigmoid(SWISH_ALPHA * gate)).astype(BF16)
            parts[e, low:high] = (
                mm(hidden, down_v[e]).astype(BF16).reshape(high - low, 2, cap, width)
            )

        run(one, 0, 2)
        for e in range(2):
            for p in range(low, high):
                part_to_mate(e, p).start()

    def chip_sum(low, high):
        for e in range(2):
            for p in range(low, high):
                part_to_mate(e, p).wait_recv()

        def add(p):
            for e in range(2):
                parts[e, p, 0] = (
                    parts[e, p, 0].astype(F32) + mate[e, p].astype(F32)
                ).astype(BF16)

        run(add, low, high)

    def plane_forward(phase):
        for i in range(2):
            for way in (1, -1):
                landed(plane(i, phase, way, 0))
                start(plane(i, phase, way, 1))

    def plane_done(phase):
        for i in range(2):
            for way in (1, -1):
                landed(plane(i, phase, way, 1))

    def gather_step(k):
        for e in range(2):
            for way in (1, -1):
                if k <= hops(way, e):
                    ring(way, e, k).wait_recv()
                    if k < hops(way, e):
                        ring(way, e, k + 1).start()
                    to_mate(e, place(-way * k)).start()

    def phase_two():
        plane_done(0)
        for i in range(2):
            for way in (1, -1):
                start(plane(i, 1, way, 0))
            start(plane_mate(i, 0))

    def norm_mix(i):
        at = pl.ds(pl.multiple_of(i * 16, 16), 16)
        normed_v[at, :] = rms_scale(mix_v[at, :], pgain_ref[...]).astype(BF16)

    def nt(a, b):
        return lax.dot_general(a, b, (((1,), (1,)), ((), ())), preferred_element_type=F32)

    rim_size = rim.shape[1]

    def glu(i):
        a = normed_v[...]
        value = nt(a, vg_all[0, i].reshape(128, width))
        gate = nt(a, vg_all[1, i].reshape(128, width))
        gated = (value * jax.nn.sigmoid(gate)).astype(BF16)
        ext[i, pl.ds(rim_size, length), :] = gated.astype(F32)
        tail_rows[i] = gated[length - rim_size :]

    rim_copy = send(tail_rows, rim, o_sem.at[0], o_sem.at[1], line_next)
    taps = taps_ref.shape[0]
    lead = rim_size - (taps - 1)
    blocks = 2
    span = length // blocks
    first = (ep + tp) == 0

    def conv(n):
        i, at = n // blocks, (n % blocks) * span
        acc = jnp.zeros((span, 128), F32)
        for r in range(8):
            picks = [j for j in range(taps) if (j + lead) % 8 == r]
            reach = max((j + lead) // 8 for j in picks) * 8
            moved = ext[i, pl.ds(at + r, span + reach), :]
            for j in picks:
                q = (j + lead) // 8 * 8
                acc = acc + taps_ref[j : j + 1, lanes(i, 128)] * moved[q : q + span]
        conv_v[pl.ds(pl.multiple_of(at, 8), span), lanes(i, 128)] = acc

    def activate(i):
        at = pl.ds(pl.multiple_of(i * 16, 16), 16)
        c = conv_v[at, :]
        c = c - jnp.mean(c, axis=-1, keepdims=True)
        var = jnp.mean(c * c, axis=-1, keepdims=True)
        c = c * lax.rsqrt(var + LAYER_EPSILON) * cgain_ref[...]
        act_v[at, :] = (c * jax.nn.sigmoid(c)).astype(BF16)

    def project(i):
        mid = act_v.shape[1] // 2
        proj_v[:, lanes(i, 256)] = mm(act_v[:, :mid], o_all[0, i]) + mm(
            act_v[:, mid:], o_all[1, i]
        )

    def norm_out(i):
        at = pl.ds(pl.multiple_of(i * 16, 16), 16)
        mixed_v[at, :] = rms_scale(proj_v[at, :], mgain_ref[...]).astype(BF16)

    def mixer_glu():
        for i in range(2):
            landed(plane_mate(i, 0))
            landed(plane_mate(i, 1))
            landed(plane_mate(i, 2))
            landed(plane_mate(i, 3))
        run(glu, 0, n_z)
        rim_copy.start()

    def mixer_conv():
        rim_copy.wait_recv()
        ext[:, :rim_size, :] = jnp.where(first, 0.0, rim[...].astype(F32))
        run(conv, 0, n_z * blocks)
        run(activate, 0, length // 16)

    mixed_copy = pltpu.make_async_copy(mixed_v, mixed_hbm, o_sem.at[2])

    def mixer_out():
        run(project, 0, n_z)
        run(norm_out, 0, length // 16)
        mixed_copy.start()

    ffn(0, 1)
    plane_forward(0)
    for k in range(1, half_z + 1):
        gather_step(k)
        if k < half_z:
            ffn(2 * k - 1, 2 * k + 1)
            if k == 1:
                phase_two()
                run(norm_mix, 0, length // 16)
            if k == half_z - 1:
                chip_sum(0, 2 * k + 1)
                for e in range(2):
                    for way in (1, -1):
                        if hops(way, e) == k:
                            ring_sum(way, e, k).start()
                plane_forward(1)
        else:
            ffn(n_z - 1, n_z)
            chip_sum(n_z - 1, n_z)

    for k in range(half_z, 0, -1):
        for e in range(2):
            for way in (1, -1):
                if k < hops(way, e):
                    ring_sum(way, e, k + 1).wait_recv()
                    p = place(way * k)
                    parts[e, p, 0] = (
                        parts[e, p, 0].astype(F32)
                        + ring_in[side[way], e, k].astype(F32)
                    ).astype(BF16)
                    ring_sum(way, e, k).start()
                elif k == half_z and hops(way, e) == k:
                    ring_sum(way, e, k).start()
        if k == half_z:
            for i in range(2):
                start(plane_mate(i, 1))
                start(plane_mate(i, 2))
            plane_done(1)
            for i in range(2):
                start(plane_mate(i, 3))
        if k == half_z - 1:
            mixer_glu()
        if k == half_z - 2:
            mixer_conv()
        if k == 1:
            mixer_out()
    done = []
    for e in range(2):
        total = parts[e, 0, 0].astype(F32)
        for way in (1, -1):
            if hops(way, e) > 0:
                ring_sum(way, e, 1).wait_recv()
                total = total + ring_in[side[way], e, 0].astype(F32)
        done.append(total.astype(BF16))

    back_rows = jnp.zeros((slots, half), F32)
    for e in range(2):
        for h in range(2):
            back_rows = back_rows + mm(
                to_rows(e, h, (slots, cap), 1, 0), done[e][:, h * half : (h + 1) * half]
            )
    back_slab[...] = back_rows.astype(BF16).reshape(n_ep, 16, half)
    back_copy = exchange(back_slab, back, b_send, b_recv)
    run(lambda i: back_copy(i).start(), 1, n_ep)
    back[ep] = back_slab[ep]
    mixes = []
    spot = [upright(s.astype(F32)).astype(jnp.int32) for s in spot_row]
    share_of = [upright(rw_ref[k : k + 1, :]) for k in range(2)]
    for h in range(2):
        at = iota((tokens, slots), 1) - 8 * h
        share = jnp.zeros((tokens, slots), F32)
        for k in range(2):
            share = share + jnp.where(at == spot[k], share_of[k], 0.0)
        high = share.astype(BF16)
        mixes.append((high, (share - high.astype(F32)).astype(BF16)))

    run(lambda i: out_copy(i).wait_send(), 1, n_ep)
    run(lambda dz: left(column_copies(dz)), 1, n_z)
    for i in range(2):
        for phase in range(2):
            for way in (1, -1):
                left(plane(i, phase, way, 0))
                left(plane(i, phase, way, 1))
        for turn in range(4):
            left(plane_mate(i, turn))
    for e in range(2):
        for way in (1, -1):
            for k in range(1, hops(way, e) + 1):
                ring(way, e, k).wait_send()
                ring_sum(way, e, k).wait_send()
        for p in range(n_z):
            to_mate(e, p).wait_send()
            part_to_mate(e, p).wait_send()
    rim_copy.wait_send()
    mixed_copy.wait()

    run(lambda i: back_copy(i).wait_recv(), 1, n_ep)
    results = back[...].reshape(slots, half)
    combined = [mm(high, results) + mm(low, results) for high, low in mixes]
    square = sum(jnp.sum(c * c, axis=1, keepdims=True) for c in combined)
    scale = lax.rsqrt(square / width + RMS_EPSILON)
    for h in range(2):
        cols = slice(h * half, (h + 1) * half)
        out_ref[:, cols] = (combined[h] * scale * egain_ref[:, cols]).astype(BF16)
    run(lambda i: back_copy(i).wait_send(), 1, n_ep)


def on_device(
    mixer_in,
    pre_gain,
    glu_value,
    glu_gate,
    conv_kernel,
    chan_gain,
    out_weight,
    mix_gain,
    expert_in,
    ffn_gain,
    routing,
    route_weight,
    gate_proj,
    up_proj,
    down_proj,
    expert_gain,
):
    n_ep, n_z = lax.axis_size("ep"), lax.axis_size("tp") // 2
    half_z = n_z // 2
    tokens, width = expert_in.shape
    length = mixer_in.shape[0]
    half, cap, hid = width // 2, n_ep * CAPS, gate_proj.shape[2]
    channels, cols = conv_kernel.shape[1], glu_value.shape[1]
    wide = out_weight.shape[1]
    rim_size = 32
    dma = pltpu.SemaphoreType.DMA
    vmem = pl.BlockSpec(memory_space=pltpu.VMEM)
    hbm = pl.BlockSpec(memory_space=pl.ANY)
    routed, mixed = pl.pallas_call(
        functools.partial(both_kernel, n_ep, n_z),
        out_shape=(
            jax.ShapeDtypeStruct((tokens, width), BF16),
            jax.ShapeDtypeStruct((length, width), BF16),
        ),
        in_specs=[vmem] * 9 + [hbm] * 7,
        out_specs=(vmem, hbm),
        scratch_shapes=[
            pltpu.VMEM((2, width, hid), BF16),
            pltpu.VMEM((2, width, hid), BF16),
            pltpu.VMEM((2, hid, width), BF16),
            pltpu.VMEM((length, width), BF16),
            pltpu.VMEM((2, cols, width), BF16),
            pltpu.VMEM((2, channels // 2, wide), BF16),
            pltpu.VMEM((n_ep, 16, half), BF16),
            pltpu.VMEM((n_ep, 16, half), BF16),
            pltpu.VMEM((2, n_z, 2, cap, width), BF16),
            pltpu.VMEM((2, n_z, 2, cap, width), BF16),
            pltpu.VMEM((2, n_z, cap, width), BF16),
            pltpu.VMEM((2, 2, half_z, cap, width), BF16),
            pltpu.VMEM((n_ep, 16, half), BF16),
            pltpu.VMEM((n_ep, 16, half), BF16),
            pltpu.VMEM((2, n_z, 2, cols, width), BF16),
            pltpu.VMEM((2, n_z, channels // 2, 2 * wide), BF16),
            pltpu.VMEM((length, width), BF16),
            pltpu.VMEM((n_z, rim_size + length, 2 * cols), F32),
            pltpu.VMEM((n_z, rim_size, 2 * cols), BF16),
            pltpu.VMEM((n_z, rim_size, 2 * cols), BF16),
            pltpu.VMEM((length, channels), F32),
            pltpu.VMEM((length, channels), BF16),
            pltpu.VMEM((length, width), F32),
            pltpu.VMEM((length, width), BF16),
            dma((7,)),
            dma((n_ep,)),
            dma((n_ep,)),
            dma((2, 2, half_z)),
            dma((2, 2, half_z)),
            dma((2, n_z)),
            dma((2, n_z)),
            dma((2, n_z)),
            dma((2, n_z)),
            dma((2, 2, half_z)),
            dma((2, 2, half_z)),
            dma((n_ep,)),
            dma((n_ep,)),
            dma((n_z, 4)),
            dma((n_z, 4)),
            dma((2, 2, 8)),
            dma((2, 2, 8)),
            dma((2, 4, 2)),
            dma((2, 4, 2)),
            dma((4,)),
            dma((3,)),
        ],
        compiler_params=pltpu.CompilerParams(
            collective_id=0, has_side_effects=True, vmem_limit_bytes=62 * 1024 * 1024
        ),
        name="both_modules",
    )(
        expert_in,
        ffn_gain.reshape(1, -1),
        routing.T,
        route_weight.T,
        expert_gain.reshape(1, -1),
        pre_gain.reshape(1, -1),
        conv_kernel,
        chan_gain.reshape(1, -1),
        mix_gain.reshape(1, -1),
        gate_proj,
        up_proj,
        down_proj,
        mixer_in,
        glu_value.T,
        glu_gate.T,
        out_weight.reshape(2, channels // 2, wide),
    )
    return (mixed, routed)


def solution(mesh):
    in_specs = (
        P(("ep", "tp"), None),
        P(),
        P(None, "tp"),
        P(None, "tp"),
        P(),
        P(),
        P(None, "tp"),
        P(),
        P(("ep", "tp"), None),
        P(),
        P(("ep", "tp"), None),
        P(("ep", "tp"), None),
        P("ep", None, "tp"),
        P("ep", None, "tp"),
        P("ep", "tp", None),
        P(),
    )
    out_specs = (P(("ep", "tp"), None), P(("ep", "tp"), None))
    return jax.shard_map(
        on_device, mesh=mesh, in_specs=in_specs, out_specs=out_specs, check_vma=False
    )
```

```python
import functools

import jax
import jax.numpy as jnp
from jax import lax
from jax.experimental import pallas as pl
from jax.experimental.pallas import tpu as pltpu
from jax.sharding import PartitionSpec as P

RMS_EPSILON = 1e-06
LAYER_EPSILON = 1e-05
CLAMP_LIMIT = 7.0
SWISH_ALPHA = 1.702
CAPS = 3
MESH = pl.DeviceIdType.MESH
F32 = jnp.float32
BF16 = jnp.bfloat16


def iota(shape, dim):
    return lax.broadcasted_iota(jnp.int32, shape, dim)


def mm(a, b):
    return jnp.dot(a, b, preferred_element_type=F32)


def rms_scale(values, gain_row):
    values = values.astype(F32)
    return (
        values
        * lax.rsqrt(jnp.mean(values * values, axis=-1, keepdims=True) + RMS_EPSILON)
        * gain_row
    )


def both_kernel(
    n_ep,
    n_z,
    x_ref,
    fgain_ref,
    route_ref,
    rw_ref,
    egain_ref,
    pgain_ref,
    taps_ref,
    cgain_ref,
    gate_hbm,
    up_hbm,
    down_hbm,
    mix_hbm,
    value_hbm,
    glu_hbm,
    ow_hbm,
    out_ref,
    mixed_hbm,
    gate_v,
    up_v,
    down_v,
    mix_v,
    loc_vg,
    loc_o,
    slab,
    arrived,
    rows,
    parts,
    mate,
    ring_in,
    back_slab,
    back,
    vg_all,
    o_all,
    normed_v,
    ext,
    conv_v,
    act_v,
    proj_v,
    mixed_v,
    w_sem,
    a_send,
    a_recv,
    g_send,
    g_recv,
    m_send,
    m_recv,
    q_send,
    q_recv,
    s_send,
    s_recv,
    b_send,
    b_recv,
    c_send,
    c_recv,
    p_send,
    p_recv,
    t_send,
    t_recv,
    h_sem,
    o_sem,
):
    half_z = n_z // 2
    n_s = 4
    tokens, width = x_ref.shape
    cap = n_ep * CAPS
    slots = n_ep * 16
    parts_n = 8
    part_w = width // parts_n
    length = mix_hbm.shape[0]
    rim_size = mix_v.shape[0] - length
    unit = width // n_ep
    o_unit = loc_o.shape[1] // n_ep
    ep, tp = lax.axis_index("ep"), lax.axis_index("tp")
    z, core = tp // 2, tp % 2
    mate_tp = 2 * z + 1 - core
    next_tp = 2 * ((z + 1) % n_z) + core
    prev_tp = 2 * ((z + n_z - 1) % n_z) + core
    toward = {1: next_tp, -1: prev_tp}
    side = {1: 0, -1: 1}
    major = (ep // n_s, ep % n_s)
    minor = (ep % n_s, ep // n_s)
    after = (tp + 1) // (2 * n_z)
    line_next = ((ep + after) % n_ep, (tp + 1) % (2 * n_z))
    behind = (2 * n_z - tp) // (2 * n_z)
    line_prev = ((ep + n_ep - behind) % n_ep, (tp + 2 * n_z - 1) % (2 * n_z))

    def pos(d):
        return 2 * d - 1 if d > 0 else -2 * d

    def place(d):
        return n_z - 1 if d in (half_z, -half_z) else pos(d)

    def cols_of(way, k):
        if k < half_z:
            return slice(0, width)
        return pl.ds(side[way] * (width // 2), width // 2)

    def send(src, dst, send_sem, recv_sem, device):
        return pltpu.make_async_remote_copy(
            src_ref=src,
            dst_ref=dst,
            send_sem=send_sem,
            recv_sem=recv_sem,
            device_id=device,
            device_id_type=MESH,
        )

    def bulk(ref, send_sem, recv_sem):
        return send(ref, ref, send_sem, recv_sem, (ep, mate_tp))

    def run(fn, low, high, unroll=1):
        def body(i, carry):
            fn(i)
            return carry

        lax.fori_loop(low, high, body, 0, unroll=unroll)

    def lanes(i, n):
        return pl.ds(pl.multiple_of(i * n, n), n)

    loads = [
        pltpu.make_async_copy(src, dst, w_sem.at[i])
        for i, (src, dst) in enumerate(
            (
                (value_hbm, loc_vg.at[0]),
                (glu_hbm, loc_vg.at[1]),
                (ow_hbm, loc_o),
                (gate_hbm, gate_v),
                (up_hbm, up_v),
                (down_hbm, down_v),
                (mix_hbm, mix_v.at[rim_size:]),
            )
        )
    ]
    for load in loads:
        load.start()

    barrier = pltpu.get_barrier_semaphore()

    def greet(device):
        pl.semaphore_signal(barrier, inc=1, device_id=device, device_id_type=MESH)

    run(lambda i: greet(((ep + i) % n_ep, tp)), 1, n_ep)
    run(lambda i: greet((ep, 2 * ((z + i) % n_z) + core)), 1, n_z)
    for device in ((ep, mate_tp), line_next, line_prev):
        greet(device)

    experts = 2 * n_ep
    eye = iota((tokens, tokens), 0) == iota((tokens, tokens), 1)

    def upright(row):
        return jnp.sum(jnp.where(eye, row, 0.0), axis=1, keepdims=True)

    chosen = [route_ref[k : k + 1, :] for k in range(2)]
    named = [(c == iota((experts, tokens), 0)).astype(F32) for c in chosen]
    earlier = (iota((tokens, tokens), 0) < iota((tokens, tokens), 1)).astype(F32)
    before = mm((named[0] + named[1]).astype(BF16), earlier.astype(BF16))
    code_row = jnp.concatenate(
        [
            c.astype(F32) * 4.0 + jnp.sum(before * n, axis=0, keepdims=True)
            for c, n in zip(chosen, named)
        ],
        axis=0,
    )
    spread = (iota((tokens, parts_n * tokens), 1) % tokens) == iota(
        (tokens, parts_n * tokens), 0
    )
    code_wide = mm(code_row.astype(BF16), spread.astype(F32).astype(BF16))
    normed = rms_scale(x_ref[...], fgain_ref[...]).astype(BF16)
    stacked = jnp.concatenate(
        [normed[:, c * part_w : (c + 1) * part_w] for c in range(parts_n)], axis=0
    )
    shape = (slots, parts_n * tokens)
    same_part = iota(shape, 0) % parts_n == iota(shape, 1) // tokens
    for slot in range(CAPS):
        key = (iota(shape, 0) // parts_n * 4 + slot).astype(F32)
        hit = (code_wide[0:1] == key) | (code_wide[1:2] == key)
        picked = mm(jnp.where(hit & same_part, 1.0, 0.0).astype(BF16), stacked)
        slab[:, :, slot * part_w : (slot + 1) * part_w] = picked.astype(BF16).reshape(
            n_ep, 16, part_w
        )
    pl.semaphore_wait(barrier, n_ep - 1 + n_z - 1 + 3)

    def exchange(src, dst, send_sem, recv_sem):
        def copy(i):
            peer = (ep + i) % n_ep
            return send(
                src.at[peer], dst.at[ep], send_sem.at[0], recv_sem.at[0], (peer, tp)
            )

        return copy

    rim_copy = send(
        mix_hbm.at[length - rim_size :],
        mix_v.at[:rim_size],
        o_sem.at[0],
        o_sem.at[1],
        line_next,
    )
    rim_copy.start()
    out_copy = exchange(slab, arrived, a_send, a_recv)
    run(lambda i: out_copy(i).start(), 1, n_ep)

    piece = [major[i] * n_s + minor[i] for i in range(2)]

    def vg_at(i, zs, who, at, count):
        return vg_all.at[zs, i, who, :, pl.ds(pl.multiple_of(at * unit, unit), count * unit)]

    def o_at(i, zs, who, at, count):
        return o_all.at[
            i, zs, pl.ds(pl.multiple_of(at * o_unit, o_unit), count * o_unit), lanes(who, 128)
        ]

    def column_copies(dz):
        device = (ep, 2 * ((z + dz) % n_z) + core)
        copies = []
        for i in range(2):
            copies.append(
                send(
                    loc_vg.at[i, :, lanes(piece[i], unit)],
                    vg_at(i, z, core, piece[i], 1),
                    c_send.at[0],
                    c_recv.at[0],
                    device,
                )
            )
            copies.append(
                send(
                    loc_o.at[i, lanes(piece[i], o_unit), :],
                    o_at(i, z, core, piece[i], 1),
                    c_send.at[1],
                    c_recv.at[1],
                    device,
                )
            )
        return copies

    own_copies = []
    for i in range(2):
        own_copies.append(
            pltpu.make_async_copy(
                loc_vg.at[i, :, lanes(piece[i], unit)],
                vg_at(i, z, core, piece[i], 1),
                h_sem.at[2 * i],
            )
        )
        own_copies.append(
            pltpu.make_async_copy(
                loc_o.at[i, lanes(piece[i], o_unit), :],
                o_at(i, z, core, piece[i], 1),
                h_sem.at[2 * i + 1],
            )
        )
    for load in loads[:3]:
        load.wait()

    def column_start(dz):
        for copy in column_copies(dz):
            copy.start()

    run(column_start, 1, n_z)
    for copy in own_copies:
        copy.start()
    arrived[ep] = slab[ep]

    def plane(i, phase, way, step):
        a, b = major[i], minor[i]
        zs = pl.ds(0, n_z) if step == 0 else pl.ds(0 if way == 1 else half_z, half_z)
        if phase == 0:
            source = (b + n_s - way * step) % n_s
            at, count = a * n_s + source, 1
            there = (a, (b + n_s + way) % n_s)
        else:
            source = (a + n_s - way * step) % n_s
            at, count = source * n_s, n_s
            there = ((a + n_s + way) % n_s, b)
        device = (there[0] * n_s + there[1] if i == 0 else there[1] * n_s + there[0], tp)
        mark = 2 * step + side[way]
        vg, o = vg_at(i, zs, core, at, count), o_at(i, zs, core, at, count)
        return [
            send(
                ref,
                ref,
                p_send.at[n],
                p_recv.at[i, phase, 2 * mark + n],
                device,
            )
            for n, ref in enumerate((vg, o))
        ]

    def plane_mate(i, turn):
        shift = (0, n_s - 1, 1, 2)[turn]
        at = ((major[i] + shift) % n_s) * n_s
        zs = pl.ds(0, n_z)
        return [
            send(ref, ref, t_send.at[n], t_recv.at[i, turn, n], (ep, mate_tp))
            for n, ref in enumerate((vg_at(i, zs, core, at, n_s), o_at(i, zs, core, at, n_s)))
        ]

    def start(copies):
        for copy in copies:
            copy.start()

    def landed(copies):
        for copy in copies:
            copy.wait_recv()

    def left(copies):
        for copy in copies:
            copy.wait_send()

    bulk(arrived.at[1:], a_send.at[0], a_recv.at[0]).wait_recv()

    def turned(across):
        turn = iota((slots, slots), 1 - across)
        hit = iota((slots, slots), across) == turn % n_ep * 16 + turn // n_ep
        return jnp.where(hit, 1.0, 0.0).astype(BF16)

    def ring(way, e, k):
        cols = cols_of(way, k)
        return send(
            rows.at[e, place(-way * (k - 1)), 0, :, cols],
            rows.at[e, place(-way * k), 0, :, cols],
            g_send.at[0],
            g_recv.at[side[way], e, k - 1],
            (ep, toward[way]),
        )

    def to_mate(e, p):
        return send(
            rows.at[e, p, 0], rows.at[e, p, 1], m_send.at[0], m_recv.at[e, p], (ep, mate_tp)
        )

    def part_to_mate(e, p):
        return send(
            parts.at[e, p, 1], mate.at[e, p], q_send.at[0], q_recv.at[e, p], (ep, mate_tp)
        )

    def ring_sum(way, e, k):
        cols = cols_of(way, k)
        return send(
            parts.at[e, place(way * k), 0, :, cols],
            ring_in.at[side[way], e, k - 1, :, cols],
            s_send.at[0],
            s_recv.at[side[way], e, k - 1],
            (ep, toward[way]),
        )

    block = arrived[...].reshape(slots, CAPS * part_w)
    block = mm(turned(1), block).astype(BF16)
    for e in range(2):
        for c in range(parts_n):
            at = (e * parts_n + c) * n_ep
            for slot in range(CAPS):
                rows[
                    e, 0, 0, slot * n_ep : (slot + 1) * n_ep, c * part_w : (c + 1) * part_w
                ] = block[at : at + n_ep, slot * part_w : (slot + 1) * part_w]
        if e == 0:
            for way in (1, -1):
                ring(way, e, 1).start()
        to_mate(e, 0).start()

    column_bulk = [
        bulk(loc_vg.at[:, :, : (n_z - 1) * unit], c_send.at[0], c_recv.at[0]),
        bulk(loc_o.at[:, : (n_z - 1) * o_unit, :], c_send.at[1], c_recv.at[1]),
    ]

    def columns_in():
        landed(column_bulk)
        for copy in own_copies:
            copy.wait()
        for i in range(2):
            for way in (1, -1):
                start(plane(i, 0, way, 0))

    for load in loads[3:]:
        load.wait()

    def ffn(e, low, high):
        for p in range(low, high):
            to_mate(e, p).wait_recv()
        count = (high - low) * 2 * cap
        block = rows[e, low:high].reshape(count, width)
        gate = jnp.minimum(mm(block, gate_v[e]), CLAMP_LIMIT)
        up = jnp.clip(mm(block, up_v[e]), -CLAMP_LIMIT, CLAMP_LIMIT)
        hidden = ((up + 1.0) * gate * jax.nn.sigmoid(SWISH_ALPHA * gate)).astype(BF16)
        parts[e, low:high] = (
            mm(hidden, down_v[e]).astype(BF16).reshape(high - low, 2, cap, width)
        )
        for p in range(low, high):
            part_to_mate(e, p).start()

    def chip_sum(e, low, high):
        for p in range(low, high):
            part_to_mate(e, p).wait_recv()

        def add(p):
            parts[e, p, 0] = (
                parts[e, p, 0].astype(F32) + mate[e, p].astype(F32)
            ).astype(BF16)

        run(add, low, high)

    def plane_forward(phase, i):
        for way in (1, -1):
            landed(plane(i, phase, way, 0))
            start(plane(i, phase, way, 1))
        if phase == 1:
            start(plane_mate(i, 1))
            start(plane_mate(i, 2))

    def phase_two(i):
        for way in (1, -1):
            landed(plane(i, 0, way, 1))
        for way in (1, -1):
            start(plane(i, 1, way, 0))
        start(plane_mate(i, 0))

    def gather_step(e, k, way):
        ring(way, e, k).wait_recv()
        if k < half_z:
            ring(way, e, k + 1).start()
            to_mate(e, place(-way * k)).start()

    def gather_far(e):
        for way in (1, -1):
            gather_step(e, half_z, way)
        to_mate(e, place(half_z)).start()

    def scatter_first(e):
        for way in (1, -1):
            ring_sum(way, e, half_z).start()

    def scatter_step(e, k, way):
        ring_sum(way, e, k + 1).wait_recv()
        p, cols = place(way * k), cols_of(way, k + 1)
        parts[e, p, 0, :, cols] = (
            parts[e, p, 0, :, cols].astype(F32)
            + ring_in[side[way], e, k, :, cols].astype(F32)
        ).astype(BF16)
        ring_sum(way, e, k).start()

    def scatter_last(e):
        total = parts[e, 0, 0].astype(F32)
        for way in (1, -1):
            ring_sum(way, e, 1).wait_recv()
            total = total + ring_in[side[way], e, 0].astype(F32)
        return total.astype(BF16)

    def norm_mix(i):
        at = pl.ds(pl.multiple_of(i * 16, 16), 16)
        normed_v[at, :] = rms_scale(mix_v[at, :], pgain_ref[...]).astype(BF16)

    def nt(a, b):
        return lax.dot_general(a, b, (((1,), (1,)), ((), ())), preferred_element_type=F32)

    def glu(i):
        a = normed_v[...]
        pre = nt(a, vg_all[i].reshape(256, width))
        gated = (pre[:, :128] * jax.nn.sigmoid(pre[:, 128:])).astype(BF16).astype(F32)
        ext[i] = jnp.where(real, gated, 0.0)

    taps = taps_ref.shape[0]
    lead = rim_size - (taps - 1)
    blocks = 2
    span = length // blocks
    real = iota((rim_size + length, 128), 0) >= jnp.where((ep + tp) == 0, rim_size, 0)

    def conv(n):
        i, at = n // blocks, (n % blocks) * span
        acc = jnp.zeros((span, 128), F32)
        for r in range(8):
            picks = [j for j in range(taps) if (j + lead) % 8 == r]
            reach = max((j + lead) // 8 for j in picks) * 8
            moved = ext[i, pl.ds(at + r, span + reach), :]
            for j in picks:
                q = (j + lead) // 8 * 8
                acc = acc + taps_ref[j : j + 1, lanes(i, 128)] * moved[q : q + span]
        conv_v[pl.ds(pl.multiple_of(at, 8), span), lanes(i, 128)] = acc

    def activate(i):
        at = pl.ds(pl.multiple_of(i * 32, 32), 32)
        c = conv_v[at, :]
        c = c - jnp.mean(c, axis=-1, keepdims=True)
        var = jnp.mean(c * c, axis=-1, keepdims=True)
        c = c * lax.rsqrt(var + LAYER_EPSILON) * cgain_ref[...]
        act_v[at, :] = (c * jax.nn.sigmoid(c)).astype(BF16)

    def project(i):
        mid = act_v.shape[1] // 2
        proj_v[:, lanes(i, 256)] = mm(act_v[:, :mid], o_all[0, i]) + mm(
            act_v[:, mid:], o_all[1, i]
        )

    def norm_out(i):
        at = pl.ds(pl.multiple_of(i * 16, 16), 16)
        mixed_v[at, :] = rms_scale(proj_v[at, :], 1.0).astype(BF16)

    def weights_out(i):
        for way in (1, -1):
            landed(plane(i, 1, way, 1))
        start(plane_mate(i, 3))

    def weights_in():
        for i in range(2):
            for turn in range(4):
                landed(plane_mate(i, turn))

    def mixer_glu(low, high):
        run(glu, low, high)

    def mixer_conv(low, high):
        run(conv, low, high)

    def mixer_act():
        run(activate, 0, length // 32, 2)

    mixed_copy = pltpu.make_async_copy(mixed_v, mixed_hbm, o_sem.at[2])

    def norm_mix_all():
        rim_copy.wait_recv()
        run(norm_mix, 0, (rim_size + length) // 16, 2)

    def mixer_out():
        run(project, 0, n_z)
        run(norm_out, 0, length // 16, 2)
        mixed_copy.start()

    ffn(0, 0, 1)
    columns_in()
    norm_mix_all()
    for way in (1, -1):
        ring(way, 1, 1).start()
    gather_step(0, 1, -1)
    gather_step(0, 1, 1)
    ffn(1, 0, 1)
    plane_forward(0, 0)
    plane_forward(0, 1)
    gather_step(1, 1, 1)
    gather_step(1, 1, -1)
    gather_step(0, 2, -1)
    gather_step(0, 2, 1)
    phase_two(0)
    phase_two(1)
    ffn(0, 1, 3)
    gather_step(1, 2, -1)
    gather_step(1, 2, 1)
    ffn(1, 1, 3)
    chip_sum(0, 0, 3)
    gather_step(0, 3, 1)
    gather_step(0, 3, -1)
    ffn(0, 3, 5)
    chip_sum(1, 0, 3)
    ffn(1, 3, 5)
    gather_step(1, 3, -1)
    gather_step(1, 3, 1)
    ffn(0, 5, 7)
    gather_far(0)
    chip_sum(0, 3, 5)
    chip_sum(1, 3, 5)
    ffn(0, 7, 8)
    chip_sum(0, 5, 7)
    gather_far(1)
    ffn(1, 5, 7)
    chip_sum(0, 7, 8)
    scatter_first(0)
    ffn(1, 7, 8)
    plane_forward(1, 0)
    plane_forward(1, 1)
    chip_sum(1, 5, 7)
    chip_sum(1, 7, 8)
    scatter_first(1)

    scatter_step(0, 3, 1)
    scatter_step(0, 3, -1)
    scatter_step(1, 3, -1)
    scatter_step(1, 3, 1)
    scatter_step(0, 2, -1)
    scatter_step(0, 2, 1)
    weights_out(0)
    weights_out(1)
    scatter_step(1, 2, -1)
    scatter_step(1, 2, 1)
    weights_in()
    mixer_glu(0, 6)
    scatter_step(0, 1, 1)
    scatter_step(0, 1, -1)
    mixer_glu(6, n_z)
    scatter_step(1, 1, 1)
    scatter_step(1, 1, -1)
    mixer_conv(0, n_z * blocks)
    done = [scatter_last(0), None]
    mixer_act()
    done[1] = scatter_last(1)

    gathered = jnp.concatenate(
        [
            jnp.concatenate(
                [
                    done[e][slot * n_ep : (slot + 1) * n_ep, c * part_w : (c + 1) * part_w]
                    for slot in range(CAPS)
                ],
                axis=1,
            )
            for e in range(2)
            for c in range(parts_n)
        ],
        axis=0,
    )
    back_slab[...] = mm(turned(0), gathered).astype(BF16).reshape(n_ep, 16, CAPS * part_w)
    back_copy = exchange(back_slab, back, b_send, b_recv)
    run(lambda i: back_copy(i).start(), 1, n_ep)
    back[ep] = back_slab[ep]
    mixer_out()
    code = [upright(code_row[k : k + 1, :]) for k in range(2)]
    share_of = [upright(rw_ref[k : k + 1, :]) for k in range(2)]
    code, share_of = (
        [jnp.concatenate([c] * parts_n, axis=0) for c in cs] for cs in (code, share_of)
    )
    shape = (parts_n * tokens, slots)
    same_part = iota(shape, 1) % parts_n == iota(shape, 0) // tokens
    mixes = []
    for slot in range(CAPS):
        key = (iota(shape, 1) // parts_n * 4 + slot).astype(F32)
        share = jnp.zeros(shape, F32)
        for k in range(2):
            share = share + jnp.where((code[k] == key) & same_part, share_of[k], 0.0)
        high = share.astype(BF16)
        mixes.append((high, (share - high.astype(F32)).astype(BF16)))

    once = [
        (arrived.at[1:], a_send.at[0]),
        (loc_vg.at[:, :, : (n_z - 1) * unit], c_send.at[0]),
        (loc_o.at[:, : (n_z - 1) * o_unit, :], c_send.at[1]),
        (vg_all.at[:, :, 0, :, : 15 * unit], p_send.at[0]),
        (o_all.at[:, :, : 15 * o_unit, :128], p_send.at[1]),
        (vg_all.at[:, :, 0], t_send.at[0]),
        (o_all.at[:, :, :, :128], t_send.at[1]),
        (rows.at[:, : n_z - 1, 0], g_send.at[0]),
        (parts.at[:, : n_z - 1, 0], s_send.at[0]),
        (rows.at[:, :, 0], m_send.at[0]),
        (parts.at[:, :, 1], q_send.at[0]),
    ]
    for ref, sem in once:
        bulk(ref, sem, o_sem.at[1]).wait_send()
    rim_copy.wait_send()
    mixed_copy.wait()

    bulk(back.at[1:], b_send.at[0], b_recv.at[0]).wait_recv()
    results = back[...].reshape(slots, CAPS * part_w)
    combined = jnp.zeros((parts_n * tokens, part_w), F32)
    for slot, (high, low) in enumerate(mixes):
        part = results[:, slot * part_w : (slot + 1) * part_w]
        combined = combined + mm(high, part) + mm(low, part)
    square = jnp.sum(combined * combined, axis=1, keepdims=True)
    square = sum(square[c * tokens : (c + 1) * tokens] for c in range(parts_n))
    scale = lax.rsqrt(square / width + RMS_EPSILON)
    for c in range(parts_n):
        cols = slice(c * part_w, (c + 1) * part_w)
        out_ref[:, cols] = (
            combined[c * tokens : (c + 1) * tokens] * scale * egain_ref[:, cols]
        ).astype(BF16)
    bulk(back.at[1:], b_send.at[0], b_recv.at[0]).wait_send()


def on_device(
    mixer_in,
    pre_gain,
    glu_value,
    glu_gate,
    conv_kernel,
    chan_gain,
    out_weight,
    mix_gain,
    expert_in,
    ffn_gain,
    routing,
    route_weight,
    gate_proj,
    up_proj,
    down_proj,
    expert_gain,
):
    n_ep, n_z = lax.axis_size("ep"), lax.axis_size("tp") // 2
    half_z = n_z // 2
    tokens, width = expert_in.shape
    length = mixer_in.shape[0]
    slab_w, cap, hid = CAPS * (width // 8), n_ep * CAPS, gate_proj.shape[2]
    channels, cols = conv_kernel.shape[1], glu_value.shape[1]
    wide = out_weight.shape[1]
    rim_size = 32
    dma = pltpu.SemaphoreType.DMA
    vmem = pl.BlockSpec(memory_space=pltpu.VMEM)
    hbm = pl.BlockSpec(memory_space=pl.ANY)
    routed, mixed = pl.pallas_call(
        functools.partial(both_kernel, n_ep, n_z),
        out_shape=(
            jax.ShapeDtypeStruct((tokens, width), BF16),
            jax.ShapeDtypeStruct((length, width), BF16),
        ),
        in_specs=[vmem] * 8 + [hbm] * 7,
        out_specs=(vmem, hbm),
        scratch_shapes=[
            pltpu.VMEM((2, width, hid), BF16),
            pltpu.VMEM((2, width, hid), BF16),
            pltpu.VMEM((2, hid, width), BF16),
            pltpu.VMEM((rim_size + length, width), BF16),
            pltpu.VMEM((2, cols, width), BF16),
            pltpu.VMEM((2, channels // 2, wide), BF16),
            pltpu.VMEM((n_ep, 16, slab_w), BF16),
            pltpu.VMEM((n_ep, 16, slab_w), BF16),
            pltpu.VMEM((2, n_z, 2, cap, width), BF16),
            pltpu.VMEM((2, n_z, 2, cap, width), BF16),
            pltpu.VMEM((2, n_z, cap, width), BF16),
            pltpu.VMEM((2, 2, half_z, cap, width), BF16),
            pltpu.VMEM((n_ep, 16, slab_w), BF16),
            pltpu.VMEM((n_ep, 16, slab_w), BF16),
            pltpu.VMEM((n_z, 2, 2, cols, width), BF16),
            pltpu.VMEM((2, n_z, channels // 2, 2 * wide), BF16),
            pltpu.VMEM((rim_size + length, width), BF16),
            pltpu.VMEM((n_z, rim_size + length, 2 * cols), F32),
            pltpu.VMEM((length, channels), F32),
            pltpu.VMEM((length, channels), BF16),
            pltpu.VMEM((length, width), F32),
            pltpu.VMEM((length, width), BF16),
            dma((7,)),
            dma((1,)),
            dma((1,)),
            dma((1,)),
            dma((2, 2, half_z)),
            dma((1,)),
            dma((2, n_z)),
            dma((1,)),
            dma((2, n_z)),
            dma((1,)),
            dma((2, 2, half_z)),
            dma((1,)),
            dma((1,)),
            dma((2,)),
            dma((2,)),
            dma((2,)),
            dma((2, 2, 8)),
            dma((2,)),
            dma((2, 4, 2)),
            dma((4,)),
            dma((3,)),
        ],
        compiler_params=pltpu.CompilerParams(
            collective_id=0, has_side_effects=True, vmem_limit_bytes=62 * 1024 * 1024
        ),
        name="both_modules",
    )(
        expert_in,
        ffn_gain.reshape(1, -1),
        routing.T,
        route_weight.T,
        expert_gain.reshape(1, -1),
        pre_gain.reshape(1, -1),
        conv_kernel,
        chan_gain.reshape(1, -1),
        gate_proj,
        up_proj,
        down_proj,
        mixer_in,
        glu_value.T,
        glu_gate.T,
        out_weight.reshape(2, channels // 2, wide),
    )
    return ((mixed.astype(F32) * mix_gain).astype(BF16), routed)


def solution(mesh):
    in_specs = (
        P(("ep", "tp"), None),
        P(),
        P(None, "tp"),
        P(None, "tp"),
        P(),
        P(),
        P(None, "tp"),
        P(),
        P(("ep", "tp"), None),
        P(),
        P(("ep", "tp"), None),
        P(("ep", "tp"), None),
        P("ep", None, "tp"),
        P("ep", None, "tp"),
        P("ep", "tp", None),
        P(),
    )
    out_specs = (P(("ep", "tp"), None), P(("ep", "tp"), None))
    return jax.shard_map(
        on_device, mesh=mesh, in_specs=in_specs, out_specs=out_specs, check_vma=False
    )
```

```python
import functools

import jax
import jax.numpy as jnp
from jax import lax
from jax.experimental import pallas as pl
from jax.experimental.pallas import tpu as pltpu
from jax.sharding import PartitionSpec as P

RMS_EPSILON = 1e-06
LAYER_EPSILON = 1e-05
CLAMP_LIMIT = 7.0
SWISH_ALPHA = 1.702
CAPS = 3
MESH = pl.DeviceIdType.MESH
F32 = jnp.float32
BF16 = jnp.bfloat16


def iota(shape, dim):
    return lax.broadcasted_iota(jnp.int32, shape, dim)


def mm(a, b):
    return jnp.dot(a, b, preferred_element_type=F32)


def rms_scale(values, gain_row):
    values = values.astype(F32)
    return (
        values
        * lax.rsqrt(jnp.mean(values * values, axis=-1, keepdims=True) + RMS_EPSILON)
        * gain_row
    )


def both_kernel(
    n_ep,
    n_z,
    x_ref,
    fgain_ref,
    route_ref,
    rw_ref,
    egain_ref,
    pgain_ref,
    taps_ref,
    cgain_ref,
    gate_hbm,
    up_hbm,
    down_hbm,
    mix_hbm,
    value_hbm,
    glu_hbm,
    ow_hbm,
    out_ref,
    mixed_ref,
    gate_v,
    up_v,
    down_v,
    mix_v,
    loc_vg,
    loc_o,
    slab,
    arrived,
    rows,
    parts,
    mate,
    ring_in,
    back_slab,
    back,
    vg_all,
    o_all,
    normed_v,
    ext,
    conv_v,
    act_v,
    proj_v,
    w_sem,
    a_send,
    a_recv,
    g_send,
    g_recv,
    m_send,
    m_recv,
    q_send,
    q_recv,
    s_send,
    s_recv,
    b_send,
    b_recv,
    c_send,
    c_recv,
    p_send,
    p_recv,
    t_send,
    t_recv,
    h_sem,
    o_sem,
):
    half_z = n_z // 2
    n_s = 4
    tokens, width = x_ref.shape
    cap = n_ep * CAPS
    slots = n_ep * 16
    parts_n = 8
    part_w = width // parts_n
    length = mix_hbm.shape[0]
    rim_size = mix_v.shape[0] - length
    unit = width // n_ep
    o_unit = loc_o.shape[1] // n_ep
    ep, tp = lax.axis_index("ep"), lax.axis_index("tp")
    z, core = tp // 2, tp % 2
    mate_tp = 2 * z + 1 - core
    next_tp = 2 * ((z + 1) % n_z) + core
    prev_tp = 2 * ((z + n_z - 1) % n_z) + core
    toward = {1: next_tp, -1: prev_tp}
    side = {1: 0, -1: 1}
    major = (ep // n_s, ep % n_s)
    minor = (ep % n_s, ep // n_s)
    after = (tp + 1) // (2 * n_z)
    line_next = ((ep + after) % n_ep, (tp + 1) % (2 * n_z))
    behind = (2 * n_z - tp) // (2 * n_z)
    line_prev = ((ep + n_ep - behind) % n_ep, (tp + 2 * n_z - 1) % (2 * n_z))

    def pos(d):
        return 2 * d - 1 if d > 0 else -2 * d

    def place(d):
        return n_z - 1 if d in (half_z, -half_z) else pos(d)

    def cols_of(way, k):
        if k < half_z:
            return slice(0, width)
        return pl.ds(side[way] * (width // 2), width // 2)

    def send(src, dst, send_sem, recv_sem, device):
        return pltpu.make_async_remote_copy(
            src_ref=src,
            dst_ref=dst,
            send_sem=send_sem,
            recv_sem=recv_sem,
            device_id=device,
            device_id_type=MESH,
        )

    def bulk(ref, send_sem, recv_sem):
        return send(ref, ref, send_sem, recv_sem, (ep, mate_tp))

    def run(fn, low, high, unroll=1):
        def body(i, carry):
            fn(i)
            return carry

        lax.fori_loop(low, high, body, 0, unroll=unroll)

    def lanes(i, n):
        return pl.ds(pl.multiple_of(i * n, n), n)

    loads = [
        pltpu.make_async_copy(src, dst, w_sem.at[i])
        for i, (src, dst) in enumerate(
            (
                (value_hbm, loc_vg.at[0]),
                (glu_hbm, loc_vg.at[1]),
                (ow_hbm, loc_o),
                (gate_hbm, gate_v),
                (up_hbm, up_v),
                (down_hbm, down_v),
                (mix_hbm, mix_v.at[rim_size:]),
            )
        )
    ]
    for load in loads:
        load.start()

    barrier = pltpu.get_barrier_semaphore()

    def greet(device):
        pl.semaphore_signal(barrier, inc=1, device_id=device, device_id_type=MESH)

    run(lambda i: greet(((ep + i) % n_ep, tp)), 1, n_ep)
    run(lambda i: greet((ep, 2 * ((z + i) % n_z) + core)), 1, n_z)
    for device in ((ep, mate_tp), line_next, line_prev):
        greet(device)

    experts = 2 * n_ep
    eye = iota((tokens, tokens), 0) == iota((tokens, tokens), 1)

    def upright(row):
        return jnp.sum(jnp.where(eye, row, 0.0), axis=1, keepdims=True)

    chosen = [route_ref[k : k + 1, :] for k in range(2)]
    named = [(c == iota((experts, tokens), 0)).astype(F32) for c in chosen]
    earlier = (iota((tokens, tokens), 0) < iota((tokens, tokens), 1)).astype(F32)
    before = mm((named[0] + named[1]).astype(BF16), earlier.astype(BF16))
    code_row = jnp.concatenate(
        [
            c.astype(F32) * 4.0 + jnp.sum(before * n, axis=0, keepdims=True)
            for c, n in zip(chosen, named)
        ],
        axis=0,
    )
    spread = (iota((tokens, parts_n * tokens), 1) % tokens) == iota(
        (tokens, parts_n * tokens), 0
    )
    code_wide = mm(code_row.astype(BF16), spread.astype(F32).astype(BF16))
    normed = rms_scale(x_ref[...], fgain_ref[...]).astype(BF16)
    stacked = jnp.concatenate(
        [normed[:, c * part_w : (c + 1) * part_w] for c in range(parts_n)], axis=0
    )
    shape = (slots, parts_n * tokens)
    same_part = iota(shape, 0) % parts_n == iota(shape, 1) // tokens
    for slot in range(CAPS):
        key = (iota(shape, 0) // parts_n * 4 + slot).astype(F32)
        hit = (code_wide[0:1] == key) | (code_wide[1:2] == key)
        picked = mm(jnp.where(hit & same_part, 1.0, 0.0).astype(BF16), stacked)
        slab[:, :, slot * part_w : (slot + 1) * part_w] = picked.astype(BF16).reshape(
            n_ep, 16, part_w
        )
    pl.semaphore_wait(barrier, n_ep - 1 + n_z - 1 + 3)

    def exchange(src, dst, send_sem, recv_sem):
        def copy(i):
            peer = (ep + i) % n_ep
            return send(
                src.at[peer], dst.at[ep], send_sem.at[0], recv_sem.at[0], (peer, tp)
            )

        return copy

    rim_copy = send(
        mix_hbm.at[length - rim_size :],
        mix_v.at[:rim_size],
        o_sem.at[0],
        o_sem.at[1],
        line_next,
    )
    rim_copy.start()
    out_copy = exchange(slab, arrived, a_send, a_recv)
    run(lambda i: out_copy(i).start(), 1, n_ep)

    piece = [major[i] * n_s + minor[i] for i in range(2)]

    def vg_at(i, zs, who, at, count):
        return vg_all.at[zs, i, who, :, pl.ds(pl.multiple_of(at * unit, unit), count * unit)]

    def o_at(i, zs, who, at, count):
        return o_all.at[
            i, zs, pl.ds(pl.multiple_of(at * o_unit, o_unit), count * o_unit), lanes(who, 128)
        ]

    def piece_from(i, n):
        if n == 0:
            return loc_vg.at[i, :, lanes(piece[i], unit)]
        return loc_o.at[i, lanes(piece[i], o_unit), :]

    def region(i, zs, at, count, n):
        return vg_at(i, zs, core, at, count) if n == 0 else o_at(i, zs, core, at, count)

    def own_copy(i, n):
        return pltpu.make_async_copy(
            piece_from(i, n), region(i, z, piece[i], 1, n), h_sem.at[2 * i + n]
        )

    def column_send(n):
        def one(dz):
            for i in range(2):
                send(
                    piece_from(i, n),
                    region(i, z, piece[i], 1, n),
                    c_send.at[n],
                    c_recv.at[n],
                    (ep, 2 * ((z + dz) % n_z) + core),
                ).start()

        run(one, 1, n_z)
        for i in range(2):
            own_copy(i, n).start()

    for load in loads[:2]:
        load.wait()
    column_send(0)
    arrived[ep] = slab[ep]

    def plane(i, phase, way, step, n):
        a, b = major[i], minor[i]
        zs = pl.ds(0, n_z) if step == 0 else pl.ds(0 if way == 1 else half_z, half_z)
        if phase == 0:
            source = (b + n_s - way * step) % n_s
            at, count = a * n_s + source, 1
            there = (a, (b + n_s + way) % n_s)
        else:
            source = (a + n_s - way * step) % n_s
            at, count = source * n_s, n_s
            there = ((a + n_s + way) % n_s, b)
        ref = region(i, zs, at, count, n)
        return send(
            ref,
            ref,
            p_send.at[n],
            p_recv.at[i, phase, 2 * (2 * step + side[way]) + n],
            (there[0] * n_s + there[1] if i == 0 else there[1] * n_s + there[0], tp),
        )

    def plane_mate(i, turn, n):
        shift = (0, n_s - 1, 1, 2)[turn]
        at = ((major[i] + shift) % n_s) * n_s
        ref = region(i, pl.ds(0, n_z), at, n_s, n)
        return send(ref, ref, t_send.at[n], t_recv.at[n], (ep, mate_tp))

    bulk(arrived.at[1:], a_send.at[0], a_recv.at[0]).wait_recv()

    def turned(across):
        turn = iota((slots, slots), 1 - across)
        hit = iota((slots, slots), across) == turn % n_ep * 16 + turn // n_ep
        return jnp.where(hit, 1.0, 0.0).astype(BF16)

    def ring(way, e, k):
        cols = cols_of(way, k)
        return send(
            rows.at[e, place(-way * (k - 1)), 0, :, cols],
            rows.at[e, place(-way * k), 0, :, cols],
            g_send.at[0],
            g_recv.at[side[way], e, k - 1],
            (ep, toward[way]),
        )

    def to_mate(e, p):
        return send(
            rows.at[e, p, 0], rows.at[e, p, 1], m_send.at[0], m_recv.at[e, p], (ep, mate_tp)
        )

    def part_to_mate(e, p):
        return send(
            parts.at[e, p, 1], mate.at[e, p], q_send.at[0], q_recv.at[e, p], (ep, mate_tp)
        )

    def ring_sum(way, e, k, early=False):
        cols, mark = cols_of(way, k), k - 1
        if k == half_z - 1:
            cols = cols_of(-way if early else way, half_z)
            mark = half_z if early else mark
        return send(
            parts.at[e, place(way * k), 0, :, cols],
            ring_in.at[side[way], e, k - 1, :, cols],
            s_send.at[0],
            s_recv.at[side[way], e, mark],
            (ep, toward[way]),
        )

    block = arrived[...].reshape(slots, CAPS * part_w)
    block = mm(turned(1), block).astype(BF16)
    for e in range(2):
        for c in range(parts_n):
            at = (e * parts_n + c) * n_ep
            for slot in range(CAPS):
                rows[
                    e, 0, 0, slot * n_ep : (slot + 1) * n_ep, c * part_w : (c + 1) * part_w
                ] = block[at : at + n_ep, slot * part_w : (slot + 1) * part_w]
        if e == 0:
            for way in (1, -1):
                ring(way, e, 1).start()
        to_mate(e, 0).start()

    column_bulk = [
        bulk(loc_vg.at[:, :, : (n_z - 1) * unit], c_send.at[0], c_recv.at[0]),
        bulk(loc_o.at[:, : (n_z - 1) * o_unit, :], c_send.at[1], c_recv.at[1]),
    ]

    def columns_in(n):
        column_bulk[n].wait_recv()
        for i in range(2):
            own_copy(i, n).wait()
        for i in range(2):
            for way in (1, -1):
                plane(i, 0, way, 0, n).start()

    for load in loads[2:]:
        load.wait()

    def ffn(e, low, high):
        for p in range(low, high):
            to_mate(e, p).wait_recv()
        count = (high - low) * 2 * cap
        block = rows[e, low:high].reshape(count, width)
        gate = jnp.minimum(mm(block, gate_v[e]), CLAMP_LIMIT)
        up = jnp.clip(mm(block, up_v[e]), -CLAMP_LIMIT, CLAMP_LIMIT)
        hidden = ((up + 1.0) * gate * jax.nn.sigmoid(SWISH_ALPHA * gate)).astype(BF16)
        parts[e, low:high] = (
            mm(hidden, down_v[e]).astype(BF16).reshape(high - low, 2, cap, width)
        )
        for p in range(low, high):
            part_to_mate(e, p).start()

    def chip_sum(e, low, high):
        for p in range(low, high):
            part_to_mate(e, p).wait_recv()

        def add(p):
            parts[e, p, 0] = (
                parts[e, p, 0].astype(F32) + mate[e, p].astype(F32)
            ).astype(BF16)

        run(add, low, high)

    def plane_forward(phase, n):
        for i in range(2):
            for way in (1, -1):
                plane(i, phase, way, 0, n).wait_recv()
                plane(i, phase, way, 1, n).start()

    def phase_two(n):
        for i in range(2):
            for way in (1, -1):
                plane(i, 0, way, 1, n).wait_recv()
            for way in (1, -1):
                plane(i, 1, way, 0, n).start()
            plane_mate(i, 0, n).start()

    def weights_out(n):
        for i in range(2):
            for way in (1, -1):
                plane(i, 1, way, 1, n).wait_recv()
            plane_mate(i, 3, n).start()

    def weights_mid(n):
        for i in range(2):
            for turn in (1, 2):
                plane_mate(i, turn, n).start()

    def gather_step(e, k, way):
        ring(way, e, k).wait_recv()
        if k < half_z:
            ring(way, e, k + 1).start()
            to_mate(e, place(-way * k)).start()

    def gather_far(e):
        for way in (1, -1):
            gather_step(e, half_z, way)
        to_mate(e, place(half_z)).start()

    def scatter_first(e):
        for way in (1, -1):
            ring_sum(way, e, half_z).start()

    def scatter_early(e):
        for way in (1, -1):
            ring_sum(way, e, half_z - 1, True).start()

    def scatter_step(e, k, way):
        ring_sum(way, e, k + 1).wait_recv()
        if k == half_z - 2:
            ring_sum(way, e, k + 1, True).wait_recv()
        p, cols = place(way * k), cols_of(way, k + 1)
        parts[e, p, 0, :, cols] = (
            parts[e, p, 0, :, cols].astype(F32)
            + ring_in[side[way], e, k, :, cols].astype(F32)
        ).astype(BF16)
        ring_sum(way, e, k).start()

    def scatter_last(e):
        total = parts[e, 0, 0].astype(F32)
        for way in (1, -1):
            ring_sum(way, e, 1).wait_recv()
            total = total + ring_in[side[way], e, 0].astype(F32)
        return total.astype(BF16)

    def norm_mix(i):
        at = pl.ds(pl.multiple_of(i * 16, 16), 16)
        normed_v[at, :] = rms_scale(mix_v[at, :], pgain_ref[...]).astype(BF16)

    def nt(a, b):
        return lax.dot_general(a, b, (((1,), (1,)), ((), ())), preferred_element_type=F32)

    def glu(i):
        a = normed_v[...]
        pre = nt(a, vg_all[i].reshape(256, width))
        gated = (pre[:, :128] * jax.nn.sigmoid(pre[:, 128:])).astype(BF16).astype(F32)
        ext[i] = jnp.where(real, gated, 0.0)

    taps = taps_ref.shape[0]
    lead = rim_size - (taps - 1)
    blocks = 2
    span = length // blocks
    real = iota((rim_size + length, 128), 0) >= jnp.where((ep + tp) == 0, rim_size, 0)

    def conv(n):
        i, at = n // blocks, (n % blocks) * span
        acc = jnp.zeros((span, 128), F32)
        for r in range(8):
            picks = [j for j in range(taps) if (j + lead) % 8 == r]
            reach = max((j + lead) // 8 for j in picks) * 8
            moved = ext[i, pl.ds(at + r, span + reach), :]
            for j in picks:
                q = (j + lead) // 8 * 8
                acc = acc + taps_ref[j : j + 1, lanes(i, 128)] * moved[q : q + span]
        conv_v[pl.ds(pl.multiple_of(at, 8), span), lanes(i, 128)] = acc

    def activate(i):
        at = pl.ds(pl.multiple_of(i * 32, 32), 32)
        c = conv_v[at, :]
        c = c - jnp.mean(c, axis=-1, keepdims=True)
        var = jnp.mean(c * c, axis=-1, keepdims=True)
        c = c * lax.rsqrt(var + LAYER_EPSILON) * cgain_ref[...]
        act_v[at, :] = (c * jax.nn.sigmoid(c)).astype(BF16)

    def project(i):
        mid = act_v.shape[1] // 2
        proj_v[:, lanes(i, 256)] = mm(act_v[:, :mid], o_all[0, i]) + mm(
            act_v[:, mid:], o_all[1, i]
        )

    def norm_out(i):
        at = pl.ds(pl.multiple_of(i * 16, 16), 16)
        mixed_ref[at, :] = rms_scale(proj_v[at, :], 1.0).astype(BF16)

    def weights_in(n):
        ref = (vg_all.at[:, :, 0], o_all.at[:, :, :, :128])[n]
        bulk(ref, t_send.at[n], t_recv.at[n]).wait_recv()

    def mixer_glu(low, high):
        run(glu, low, high)

    def mixer_conv(low, high):
        run(conv, low, high)

    def mixer_act():
        run(activate, 0, length // 32, 2)

    def norm_mix_all():
        rim_copy.wait_recv()
        run(norm_mix, 0, (rim_size + length) // 16, 2)

    def mixer_out():
        run(project, n_z // 2, n_z)
        run(norm_out, 0, length // 16, 2)

    ffn(0, 0, 1)
    columns_in(0)
    norm_mix_all()
    for way in (1, -1):
        ring(way, 1, 1).start()
    gather_step(0, 1, -1)
    gather_step(0, 1, 1)
    ffn(1, 0, 1)
    plane_forward(0, 0)
    gather_step(1, 1, 1)
    gather_step(1, 1, -1)
    gather_step(0, 2, -1)
    gather_step(0, 2, 1)
    phase_two(0)
    ffn(0, 1, 3)
    gather_step(1, 2, -1)
    gather_step(1, 2, 1)
    ffn(1, 1, 3)
    chip_sum(0, 0, 3)
    gather_step(0, 3, 1)
    gather_step(0, 3, -1)
    ffn(0, 3, 5)
    chip_sum(1, 0, 3)
    ffn(1, 3, 5)
    gather_step(1, 3, -1)
    gather_step(1, 3, 1)
    column_send(1)
    ffn(0, 5, 7)
    ffn(1, 5, 7)
    gather_far(0)
    chip_sum(0, 5, 7)
    scatter_early(0)
    plane_forward(1, 0)
    chip_sum(0, 3, 5)
    chip_sum(1, 3, 5)
    ffn(0, 7, 8)
    gather_far(1)
    chip_sum(1, 5, 7)
    chip_sum(0, 7, 8)
    scatter_first(0)
    scatter_early(1)
    ffn(1, 7, 8)
    chip_sum(1, 7, 8)
    scatter_first(1)
    weights_mid(0)
    columns_in(1)

    scatter_step(0, 3, 1)
    scatter_step(0, 3, -1)
    plane_forward(0, 1)
    scatter_step(1, 3, -1)
    scatter_step(1, 3, 1)
    weights_out(0)
    phase_two(1)
    scatter_step(0, 2, -1)
    scatter_step(0, 2, 1)
    weights_in(0)
    mixer_glu(0, 4)
    scatter_step(1, 2, -1)
    scatter_step(1, 2, 1)
    mixer_glu(4, n_z)
    mixer_conv(0, n_z * blocks)
    scatter_step(0, 1, 1)
    scatter_step(0, 1, -1)
    plane_forward(1, 1)
    weights_mid(1)
    mixer_act()
    scatter_step(1, 1, 1)
    scatter_step(1, 1, -1)

    group = n_ep * parts_n
    turn = iota((group, group), 1)
    hit = iota((group, group), 0) == turn % n_ep * parts_n + turn // n_ep
    turn_back = jnp.where(hit, 1.0, 0.0).astype(BF16)

    def back_copy(e, i):
        peer = (ep + i) % n_ep
        return send(
            back_slab.at[e, peer], back.at[e, ep], b_send.at[e], b_recv.at[e], (peer, tp)
        )

    def send_back(e):
        done = scatter_last(e)
        gathered = jnp.concatenate(
            [
                jnp.concatenate(
                    [
                        done[slot * n_ep : (slot + 1) * n_ep, c * part_w : (c + 1) * part_w]
                        for slot in range(CAPS)
                    ],
                    axis=1,
                )
                for c in range(parts_n)
            ],
            axis=0,
        )
        back_slab[e] = mm(turn_back, gathered).astype(BF16).reshape(
            n_ep, parts_n, CAPS * part_w
        )
        run(lambda i: back_copy(e, i).start(), 1, n_ep)
        back[e, ep] = back_slab[e, ep]

    weights_out(1)
    send_back(0)
    weights_in(1)
    run(project, 0, n_z // 2)
    send_back(1)
    mixer_out()
    code = [upright(code_row[k : k + 1, :]) for k in range(2)]
    share_of = [upright(rw_ref[k : k + 1, :]) for k in range(2)]
    code, share_of = (
        [jnp.concatenate([c] * parts_n, axis=0) for c in cs] for cs in (code, share_of)
    )
    shape = (parts_n * tokens, group)
    same_part = iota(shape, 1) % parts_n == iota(shape, 0) // tokens
    mixes = []
    for e in range(2):
        for slot in range(CAPS):
            key = (iota(shape, 1) // parts_n * 8 + 4 * e + slot).astype(F32)
            share = jnp.zeros(shape, F32)
            for k in range(2):
                share = share + jnp.where((code[k] == key) & same_part, share_of[k], 0.0)
            high = share.astype(BF16)
            mixes.append((high, (share - high.astype(F32)).astype(BF16)))

    once = [
        (arrived.at[1:], a_send.at[0]),
        (loc_vg.at[:, :, : (n_z - 1) * unit], c_send.at[0]),
        (loc_o.at[:, : (n_z - 1) * o_unit, :], c_send.at[1]),
        (vg_all.at[:, :, 0, :, : 15 * unit], p_send.at[0]),
        (o_all.at[:, :, : 15 * o_unit, :128], p_send.at[1]),
        (vg_all.at[:, :, 0], t_send.at[0]),
        (o_all.at[:, :, :, :128], t_send.at[1]),
        (rows.at[:, : n_z - 1, 0], g_send.at[0]),
        (parts.at[:, : n_z - 1, 0], s_send.at[0]),
        (rows.at[:, :, 0], m_send.at[0]),
        (parts.at[:, :, 1], q_send.at[0]),
    ]
    for ref, sem in once:
        bulk(ref, sem, o_sem.at[1]).wait_send()
    rim_copy.wait_send()

    combined = jnp.zeros((parts_n * tokens, part_w), F32)
    for e in range(2):
        bulk(back.at[e, 1:], b_send.at[e], b_recv.at[e]).wait_recv()
        results = back[e].reshape(group, CAPS * part_w)
        for slot in range(CAPS):
            high, low = mixes[e * CAPS + slot]
            part = results[:, slot * part_w : (slot + 1) * part_w]
            combined = combined + mm(high, part) + mm(low, part)
    square = jnp.sum(combined * combined, axis=1, keepdims=True)
    square = sum(square[c * tokens : (c + 1) * tokens] for c in range(parts_n))
    scale = lax.rsqrt(square / width + RMS_EPSILON)
    for c in range(parts_n):
        cols = slice(c * part_w, (c + 1) * part_w)
        out_ref[:, cols] = (
            combined[c * tokens : (c + 1) * tokens] * scale * egain_ref[:, cols]
        ).astype(BF16)
    for e in range(2):
        bulk(back.at[e, 1:], b_send.at[e], b_recv.at[e]).wait_send()


def on_device(
    mixer_in,
    pre_gain,
    glu_value,
    glu_gate,
    conv_kernel,
    chan_gain,
    out_weight,
    mix_gain,
    expert_in,
    ffn_gain,
    routing,
    route_weight,
    gate_proj,
    up_proj,
    down_proj,
    expert_gain,
):
    n_ep, n_z = lax.axis_size("ep"), lax.axis_size("tp") // 2
    half_z = n_z // 2
    tokens, width = expert_in.shape
    length = mixer_in.shape[0]
    slab_w, cap, hid = CAPS * (width // 8), n_ep * CAPS, gate_proj.shape[2]
    channels, cols = conv_kernel.shape[1], glu_value.shape[1]
    wide = out_weight.shape[1]
    rim_size = 32
    dma = pltpu.SemaphoreType.DMA
    vmem = pl.BlockSpec(memory_space=pltpu.VMEM)
    hbm = pl.BlockSpec(memory_space=pl.ANY)
    routed, mixed = pl.pallas_call(
        functools.partial(both_kernel, n_ep, n_z),
        out_shape=(
            pltpu.VMEM((tokens, width), BF16),
            pltpu.VMEM((length, width), BF16),
        ),
        in_specs=[vmem] * 8 + [hbm] * 7,
        out_specs=(vmem, vmem),
        scratch_shapes=[
            pltpu.VMEM((2, width, hid), BF16),
            pltpu.VMEM((2, width, hid), BF16),
            pltpu.VMEM((2, hid, width), BF16),
            pltpu.VMEM((rim_size + length, width), BF16),
            pltpu.VMEM((2, cols, width), BF16),
            pltpu.VMEM((2, channels // 2, wide), BF16),
            pltpu.VMEM((n_ep, 16, slab_w), BF16),
            pltpu.VMEM((n_ep, 16, slab_w), BF16),
            pltpu.VMEM((2, n_z, 2, cap, width), BF16),
            pltpu.VMEM((2, n_z, 2, cap, width), BF16),
            pltpu.VMEM((2, n_z, cap, width), BF16),
            pltpu.VMEM((2, 2, half_z, cap, width), BF16),
            pltpu.VMEM((2, n_ep, 8, slab_w), BF16),
            pltpu.VMEM((2, n_ep, 8, slab_w), BF16),
            pltpu.VMEM((n_z, 2, 2, cols, width), BF16),
            pltpu.VMEM((2, n_z, channels // 2, 2 * wide), BF16),
            pltpu.VMEM((rim_size + length, width), BF16),
            pltpu.VMEM((n_z, rim_size + length, 2 * cols), F32),
            pltpu.VMEM((length, channels), F32),
            pltpu.VMEM((length, channels), BF16),
            pltpu.VMEM((length, width), F32),
            dma((7,)),
            dma((1,)),
            dma((1,)),
            dma((1,)),
            dma((2, 2, half_z)),
            dma((1,)),
            dma((2, n_z)),
            dma((1,)),
            dma((2, n_z)),
            dma((1,)),
            dma((2, 2, half_z + 1)),
            dma((2,)),
            dma((2,)),
            dma((2,)),
            dma((2,)),
            dma((2,)),
            dma((2, 2, 8)),
            dma((2,)),
            dma((2,)),
            dma((4,)),
            dma((2,)),
        ],
        compiler_params=pltpu.CompilerParams(
            collective_id=0, has_side_effects=True, vmem_limit_bytes=60 * 1024 * 1024
        ),
        name="both_modules",
    )(
        expert_in,
        ffn_gain.reshape(1, -1),
        routing.T,
        route_weight.T,
        expert_gain.reshape(1, -1),
        pre_gain.reshape(1, -1),
        conv_kernel,
        chan_gain.reshape(1, -1),
        gate_proj,
        up_proj,
        down_proj,
        mixer_in,
        glu_value.T,
        glu_gate.T,
        out_weight.reshape(2, channels // 2, wide),
    )
    return ((mixed.astype(F32) * mix_gain).astype(BF16), routed)


def solution(mesh):
    in_specs = (
        P(("ep", "tp"), None),
        P(),
        P(None, "tp"),
        P(None, "tp"),
        P(),
        P(),
        P(None, "tp"),
        P(),
        P(("ep", "tp"), None),
        P(),
        P(("ep", "tp"), None),
        P(("ep", "tp"), None),
        P("ep", None, "tp"),
        P("ep", None, "tp"),
        P("ep", "tp", None),
        P(),
    )
    out_specs = (P(("ep", "tp"), None), P(("ep", "tp"), None))
    return jax.shard_map(
        on_device, mesh=mesh, in_specs=in_specs, out_specs=out_specs, check_vma=False
    )
```

```python
import functools

import jax
import jax.numpy as jnp
from jax import lax
from jax.experimental import pallas as pl
from jax.experimental.pallas import tpu as pltpu
from jax.sharding import PartitionSpec as P

RMS_EPSILON = 1e-06
LAYER_EPSILON = 1e-05
CLAMP_LIMIT = 7.0
SWISH_ALPHA = 1.702
CAPS = 3
MESH = pl.DeviceIdType.MESH
F32 = jnp.float32
BF16 = jnp.bfloat16


def iota(shape, dim):
    return lax.broadcasted_iota(jnp.int32, shape, dim)


def mm(a, b):
    return jnp.dot(a, b, preferred_element_type=F32)


def rms_scale(values, gain_row):
    values = values.astype(F32)
    return (
        values
        * lax.rsqrt(jnp.mean(values * values, axis=-1, keepdims=True) + RMS_EPSILON)
        * gain_row
    )


def both_kernel(
    n_ep,
    n_z,
    x_ref,
    fgain_ref,
    route_ref,
    rw_ref,
    egain_ref,
    pgain_ref,
    taps_ref,
    cgain_ref,
    gate_hbm,
    up_hbm,
    down_hbm,
    mix_hbm,
    value_hbm,
    glu_hbm,
    ow_hbm,
    out_ref,
    mixed_ref,
    gate_v,
    up_v,
    down_v,
    mix_v,
    loc_vg,
    loc_o,
    slab,
    arrived,
    rows,
    parts,
    mate,
    ring_in,
    back_slab,
    back,
    vg_all,
    o_all,
    normed_v,
    ext,
    conv_v,
    act_v,
    proj_v,
    w_sem,
    a_send,
    a_recv,
    g_send,
    g_recv,
    m_send,
    m_recv,
    q_send,
    q_recv,
    s_send,
    s_recv,
    b_send,
    b_recv,
    c_send,
    c_recv,
    p_send,
    p_recv,
    t_send,
    t_recv,
    h_sem,
    o_sem,
):
    half_z = n_z // 2
    n_s = 4
    tokens, width = x_ref.shape
    cap = n_ep * CAPS
    slots = n_ep * 16
    parts_n = 8
    part_w = width // parts_n
    length = mix_hbm.shape[0]
    rim_size = mix_v.shape[0] - length
    unit = width // n_ep
    o_unit = loc_o.shape[1] // n_ep
    ep, tp = lax.axis_index("ep"), lax.axis_index("tp")
    z, core = tp // 2, tp % 2
    mate_tp = 2 * z + 1 - core
    next_tp = 2 * ((z + 1) % n_z) + core
    prev_tp = 2 * ((z + n_z - 1) % n_z) + core
    toward = {1: next_tp, -1: prev_tp}
    side = {1: 0, -1: 1}
    major = (ep // n_s, ep % n_s)
    minor = (ep % n_s, ep // n_s)
    after = (tp + 1) // (2 * n_z)
    line_next = ((ep + after) % n_ep, (tp + 1) % (2 * n_z))
    behind = (2 * n_z - tp) // (2 * n_z)
    line_prev = ((ep + n_ep - behind) % n_ep, (tp + 2 * n_z - 1) % (2 * n_z))

    def pos(d):
        return 2 * d - 1 if d > 0 else -2 * d

    def place(d):
        return n_z - 1 if d in (half_z, -half_z) else pos(d)

    def cols_of(way, k):
        if k < half_z:
            return slice(0, width)
        return pl.ds(side[way] * (width // 2), width // 2)

    def send(src, dst, send_sem, recv_sem, device):
        return pltpu.make_async_remote_copy(
            src_ref=src,
            dst_ref=dst,
            send_sem=send_sem,
            recv_sem=recv_sem,
            device_id=device,
            device_id_type=MESH,
        )

    def bulk(ref, send_sem, recv_sem):
        return send(ref, ref, send_sem, recv_sem, (ep, mate_tp))

    def run(fn, low, high, unroll=1):
        def body(i, carry):
            fn(i)
            return carry

        lax.fori_loop(low, high, body, 0, unroll=unroll)

    def lanes(i, n):
        return pl.ds(pl.multiple_of(i * n, n), n)

    loads = [
        pltpu.make_async_copy(src, dst, w_sem.at[i])
        for i, (src, dst) in enumerate(
            (
                (value_hbm, loc_vg.at[0]),
                (glu_hbm, loc_vg.at[1]),
                (ow_hbm, loc_o),
                (gate_hbm, gate_v),
                (up_hbm, up_v),
                (down_hbm, down_v),
                (mix_hbm, mix_v.at[rim_size:]),
            )
        )
    ]
    for load in loads:
        load.start()

    barrier = pltpu.get_barrier_semaphore()

    def greet(device):
        pl.semaphore_signal(barrier, inc=1, device_id=device, device_id_type=MESH)

    run(lambda i: greet(((ep + i) % n_ep, tp)), 1, n_ep)
    run(lambda i: greet((ep, 2 * ((z + i) % n_z) + core)), 1, n_z)
    for device in ((ep, mate_tp), line_next, line_prev):
        greet(device)

    experts = 2 * n_ep
    eye = iota((tokens, tokens), 0) == iota((tokens, tokens), 1)

    def upright(row):
        return jnp.sum(jnp.where(eye, row, 0.0), axis=1, keepdims=True)

    chosen = [route_ref[k : k + 1, :] for k in range(2)]
    named = [(c == iota((experts, tokens), 0)).astype(F32) for c in chosen]
    earlier = (iota((tokens, tokens), 0) < iota((tokens, tokens), 1)).astype(F32)
    before = mm((named[0] + named[1]).astype(BF16), earlier.astype(BF16))
    code_row = jnp.concatenate(
        [
            c.astype(F32) * 4.0 + jnp.sum(before * n, axis=0, keepdims=True)
            for c, n in zip(chosen, named)
        ],
        axis=0,
    )
    spread = (iota((tokens, parts_n * tokens), 1) % tokens) == iota(
        (tokens, parts_n * tokens), 0
    )
    code_wide = mm(code_row.astype(BF16), spread.astype(F32).astype(BF16))
    normed = rms_scale(x_ref[...], fgain_ref[...]).astype(BF16)
    stacked = jnp.concatenate(
        [normed[:, c * part_w : (c + 1) * part_w] for c in range(parts_n)], axis=0
    )
    group = n_ep * parts_n
    shape = (group, parts_n * tokens)
    same_part = iota(shape, 0) % parts_n == iota(shape, 1) // tokens
    for e in range(2):
        for slot in range(CAPS):
            key = (iota(shape, 0) // parts_n * 8 + 4 * e + slot).astype(F32)
            hit = (code_wide[0:1] == key) | (code_wide[1:2] == key)
            picked = mm(jnp.where(hit & same_part, 1.0, 0.0).astype(BF16), stacked)
            slab[e, :, :, slot * part_w : (slot + 1) * part_w] = picked.astype(
                BF16
            ).reshape(n_ep, parts_n, part_w)
    pl.semaphore_wait(barrier, n_ep - 1 + n_z - 1 + 3)

    offsets = sorted(
        [(dy, dx) for dy in range(n_s) for dx in range(n_s) if dy or dx],
        key=lambda d: -(min(d[0], n_s - d[0]) + min(d[1], n_s - d[1])),
    )

    def exchange(src, dst, send_sem, recv_sem, e):
        for dy, dx in offsets:
            peer = ((ep // n_s + dy) % n_s) * n_s + (ep % n_s + dx) % n_s
            send(
                src.at[e, peer], dst.at[e, ep], send_sem.at[e], recv_sem.at[e], (peer, tp)
            ).start()

    rim_copy = send(
        mix_hbm.at[length - rim_size :],
        mix_v.at[:rim_size],
        o_sem.at[0],
        o_sem.at[1],
        line_next,
    )
    for e in range(2):
        exchange(slab, arrived, a_send, a_recv, e)

    piece = [major[i] * n_s + minor[i] for i in range(2)]

    def vg_at(i, zs, who, at, count):
        return vg_all.at[zs, i, who, :, pl.ds(pl.multiple_of(at * unit, unit), count * unit)]

    def o_at(i, zs, who, at, count):
        return o_all.at[
            i, zs, pl.ds(pl.multiple_of(at * o_unit, o_unit), count * o_unit), lanes(who, 128)
        ]

    def piece_from(i, n):
        if n == 0:
            return loc_vg.at[i, :, lanes(piece[i], unit)]
        return loc_o.at[i, lanes(piece[i], o_unit), :]

    def region(i, zs, at, count, n):
        return vg_at(i, zs, core, at, count) if n == 0 else o_at(i, zs, core, at, count)

    def own_copy(i, n):
        return pltpu.make_async_copy(
            piece_from(i, n), region(i, z, piece[i], 1, n), h_sem.at[2 * i + n]
        )

    def column_send(n):
        def one(dz):
            for i in range(2):
                send(
                    piece_from(i, n),
                    region(i, z, piece[i], 1, n),
                    c_send.at[n],
                    c_recv.at[n],
                    (ep, 2 * ((z + dz) % n_z) + core),
                ).start()

        run(one, 1, n_z)
        for i in range(2):
            own_copy(i, n).start()

    for load in loads[:2]:
        load.wait()
    column_send(0)
    rim_copy.start()
    for e in range(2):
        arrived[e, ep] = slab[e, ep]

    def plane(i, phase, way, step, n):
        a, b = major[i], minor[i]
        zs = pl.ds(0, n_z) if step == 0 else pl.ds(0 if way == 1 else half_z, half_z)
        if phase == 0:
            source = (b + n_s - way * step) % n_s
            at, count = a * n_s + source, 1
            there = (a, (b + n_s + way) % n_s)
        else:
            source = (a + n_s - way * step) % n_s
            at, count = source * n_s, n_s
            there = ((a + n_s + way) % n_s, b)
        ref = region(i, zs, at, count, n)
        return send(
            ref,
            ref,
            p_send.at[n],
            p_recv.at[i, phase, 2 * (2 * step + side[way]) + n],
            (there[0] * n_s + there[1] if i == 0 else there[1] * n_s + there[0], tp),
        )

    def plane_mate(i, turn, n):
        shift = (0, n_s - 1, 1, 2)[turn]
        at = ((major[i] + shift) % n_s) * n_s
        ref = region(i, pl.ds(0, n_z), at, n_s, n)
        return send(ref, ref, t_send.at[n], t_recv.at[n], (ep, mate_tp))


    def turned(across):
        turn = iota((group, group), 1 - across)
        hit = iota((group, group), across) == turn % n_ep * parts_n + turn // n_ep
        return jnp.where(hit, 1.0, 0.0).astype(BF16)

    def ring(way, e, k):
        cols = cols_of(way, k)
        return send(
            rows.at[e, place(-way * (k - 1)), 0, :, cols],
            rows.at[e, place(-way * k), 0, :, cols],
            g_send.at[0],
            g_recv.at[side[way], e, k - 1],
            (ep, toward[way]),
        )

    def to_mate(e, p):
        return send(
            rows.at[e, p, 0], rows.at[e, p, 1], m_send.at[0], m_recv.at[e, p], (ep, mate_tp)
        )

    def part_to_mate(e, p):
        return send(
            parts.at[e, p, 1], mate.at[e, p], q_send.at[0], q_recv.at[e, p], (ep, mate_tp)
        )

    def ring_sum(way, e, k, early=False):
        cols, mark = cols_of(way, k), k - 1
        if k == half_z - 1:
            cols = cols_of(-way if early else way, half_z)
            mark = half_z if early else mark
        return send(
            parts.at[e, place(way * k), 0, :, cols],
            ring_in.at[side[way], e, k - 1, :, cols],
            s_send.at[0],
            s_recv.at[side[way], e, mark],
            (ep, toward[way]),
        )

    turn_in = turned(1)

    def take_in(e):
        bulk(arrived.at[e, 1:], a_send.at[e], a_recv.at[e]).wait_recv()
        block = mm(turn_in, arrived[e].reshape(group, CAPS * part_w)).astype(BF16)
        for c in range(parts_n):
            at = c * n_ep
            for slot in range(CAPS):
                rows[
                    e, 0, 0, slot * n_ep : (slot + 1) * n_ep, c * part_w : (c + 1) * part_w
                ] = block[at : at + n_ep, slot * part_w : (slot + 1) * part_w]
        if e == 0:
            for way in (1, -1):
                ring(way, e, 1).start()
        to_mate(e, 0).start()

    take_in(0)
    take_in(1)

    column_bulk = [
        bulk(loc_vg.at[:, :, : (n_z - 1) * unit], c_send.at[0], c_recv.at[0]),
        bulk(loc_o.at[:, : (n_z - 1) * o_unit, :], c_send.at[1], c_recv.at[1]),
    ]

    def columns_in(n):
        column_bulk[n].wait_recv()
        for i in range(2):
            own_copy(i, n).wait()
        for i in range(2):
            for way in (1, -1):
                plane(i, 0, way, 0, n).start()

    for load in loads[2:]:
        load.wait()

    def ffn(e, low, high):
        for p in range(low, high):
            to_mate(e, p).wait_recv()
        count = (high - low) * 2 * cap
        block = rows[e, low:high].reshape(count, width)
        gate = jnp.minimum(mm(block, gate_v[e]), CLAMP_LIMIT)
        up = jnp.clip(mm(block, up_v[e]), -CLAMP_LIMIT, CLAMP_LIMIT)
        hidden = ((up + 1.0) * gate * jax.nn.sigmoid(SWISH_ALPHA * gate)).astype(BF16)
        parts[e, low:high] = (
            mm(hidden, down_v[e]).astype(BF16).reshape(high - low, 2, cap, width)
        )
        for p in range(low, high):
            part_to_mate(e, p).start()

    def chip_sum(e, low, high):
        for p in range(low, high):
            part_to_mate(e, p).wait_recv()

        def add(p):
            parts[e, p, 0] = (
                parts[e, p, 0].astype(F32) + mate[e, p].astype(F32)
            ).astype(BF16)

        run(add, low, high)

    def plane_forward(phase, n):
        for i in range(2):
            for way in (1, -1):
                plane(i, phase, way, 0, n).wait_recv()
                plane(i, phase, way, 1, n).start()

    def phase_two(n):
        for i in range(2):
            for way in (1, -1):
                plane(i, 0, way, 1, n).wait_recv()
            for way in (1, -1):
                plane(i, 1, way, 0, n).start()
            plane_mate(i, 0, n).start()

    def weights_out(n):
        for i in range(2):
            for way in (1, -1):
                plane(i, 1, way, 1, n).wait_recv()
            plane_mate(i, 3, n).start()

    def weights_mid(n):
        for i in range(2):
            for turn in (1, 2):
                plane_mate(i, turn, n).start()

    def gather_step(e, k, way):
        ring(way, e, k).wait_recv()
        if k < half_z:
            ring(way, e, k + 1).start()
            to_mate(e, place(-way * k)).start()

    def gather_far(e):
        for way in (1, -1):
            gather_step(e, half_z, way)
        to_mate(e, place(half_z)).start()

    def scatter_first(e):
        for way in (1, -1):
            ring_sum(way, e, half_z).start()

    def scatter_early(e):
        for way in (1, -1):
            ring_sum(way, e, half_z - 1, True).start()

    def scatter_step(e, k, way):
        ring_sum(way, e, k + 1).wait_recv()
        if k == half_z - 2:
            ring_sum(way, e, k + 1, True).wait_recv()
        p, cols = place(way * k), cols_of(way, k + 1)
        parts[e, p, 0, :, cols] = (
            parts[e, p, 0, :, cols].astype(F32)
            + ring_in[side[way], e, k, :, cols].astype(F32)
        ).astype(BF16)
        ring_sum(way, e, k).start()

    def scatter_last(e):
        total = parts[e, 0, 0].astype(F32)
        for way in (1, -1):
            ring_sum(way, e, 1).wait_recv()
            total = total + ring_in[side[way], e, 0].astype(F32)
        return total.astype(BF16)

    def norm_mix(i):
        at = pl.ds(pl.multiple_of(i * 16, 16), 16)
        normed_v[at, :] = rms_scale(mix_v[at, :], pgain_ref[...]).astype(BF16)

    def nt(a, b):
        return lax.dot_general(a, b, (((1,), (1,)), ((), ())), preferred_element_type=F32)

    def glu(i):
        a = normed_v[...]
        pre = nt(a, vg_all[i].reshape(256, width))
        gated = (pre[:, :128] * jax.nn.sigmoid(pre[:, 128:])).astype(BF16).astype(F32)
        ext[i] = jnp.where(real, gated, 0.0)

    taps = taps_ref.shape[0]
    lead = rim_size - (taps - 1)
    blocks = 2
    span = length // blocks
    real = iota((rim_size + length, 128), 0) >= jnp.where((ep + tp) == 0, rim_size, 0)

    def conv(n):
        i, at = n // blocks, (n % blocks) * span
        acc = jnp.zeros((span, 128), F32)
        for r in range(8):
            picks = [j for j in range(taps) if (j + lead) % 8 == r]
            reach = max((j + lead) // 8 for j in picks) * 8
            moved = ext[i, pl.ds(at + r, span + reach), :]
            for j in picks:
                q = (j + lead) // 8 * 8
                acc = acc + taps_ref[j : j + 1, lanes(i, 128)] * moved[q : q + span]
        conv_v[pl.ds(pl.multiple_of(at, 8), span), lanes(i, 128)] = acc

    def activate(i):
        at = pl.ds(pl.multiple_of(i * 32, 32), 32)
        c = conv_v[at, :]
        c = c - jnp.mean(c, axis=-1, keepdims=True)
        var = jnp.mean(c * c, axis=-1, keepdims=True)
        c = c * lax.rsqrt(var + LAYER_EPSILON) * cgain_ref[...]
        act_v[at, :] = (c * jax.nn.sigmoid(c)).astype(BF16)

    def project(i):
        mid = act_v.shape[1] // 2
        proj_v[:, lanes(i, 256)] = mm(act_v[:, :mid], o_all[0, i]) + mm(
            act_v[:, mid:], o_all[1, i]
        )

    def norm_out(i):
        at = pl.ds(pl.multiple_of(i * 16, 16), 16)
        mixed_ref[at, :] = rms_scale(proj_v[at, :], 1.0).astype(BF16)

    def weights_in(n):
        ref = (vg_all.at[:, :, 0], o_all.at[:, :, :, :128])[n]
        bulk(ref, t_send.at[n], t_recv.at[n]).wait_recv()

    def mixer_glu(low, high):
        run(glu, low, high)

    def mixer_conv(low, high):
        run(conv, low, high)

    def mixer_act():
        run(activate, 0, length // 32, 2)

    def norm_mix_all():
        rim_copy.wait_recv()
        run(norm_mix, 0, (rim_size + length) // 16, 2)

    def mixer_out():
        run(project, n_z // 2, n_z)
        run(norm_out, 0, length // 16, 2)

    ffn(0, 0, 1)
    columns_in(0)
    norm_mix_all()
    for way in (1, -1):
        ring(way, 1, 1).start()
    gather_step(0, 1, -1)
    gather_step(0, 1, 1)
    ffn(1, 0, 1)
    plane_forward(0, 0)
    gather_step(1, 1, 1)
    gather_step(1, 1, -1)
    gather_step(0, 2, -1)
    gather_step(0, 2, 1)
    phase_two(0)
    ffn(0, 1, 3)
    gather_step(1, 2, -1)
    gather_step(1, 2, 1)
    ffn(1, 1, 3)
    chip_sum(0, 0, 3)
    gather_step(0, 3, 1)
    gather_step(0, 3, -1)
    ffn(0, 3, 5)
    chip_sum(1, 0, 3)
    ffn(1, 3, 5)
    gather_step(1, 3, -1)
    gather_step(1, 3, 1)
    column_send(1)
    ffn(0, 5, 7)
    ffn(1, 5, 7)
    gather_far(0)
    chip_sum(0, 5, 7)
    scatter_early(0)
    plane_forward(1, 0)
    chip_sum(0, 3, 5)
    chip_sum(1, 3, 5)
    ffn(0, 7, 8)
    gather_far(1)
    chip_sum(1, 5, 7)
    chip_sum(0, 7, 8)
    scatter_first(0)
    scatter_early(1)
    ffn(1, 7, 8)
    chip_sum(1, 7, 8)
    scatter_first(1)
    weights_mid(0)
    columns_in(1)

    scatter_step(0, 3, 1)
    scatter_step(0, 3, -1)
    plane_forward(0, 1)
    scatter_step(1, 3, -1)
    scatter_step(1, 3, 1)
    weights_out(0)
    phase_two(1)
    scatter_step(0, 2, -1)
    scatter_step(0, 2, 1)
    weights_in(0)
    mixer_glu(0, 4)
    scatter_step(1, 2, -1)
    scatter_step(1, 2, 1)
    mixer_glu(4, n_z)
    mixer_conv(0, n_z * blocks)
    scatter_step(0, 1, 1)
    scatter_step(0, 1, -1)
    plane_forward(1, 1)
    weights_mid(1)
    mixer_act()
    scatter_step(1, 1, 1)
    scatter_step(1, 1, -1)

    turn_back = turned(0)

    def send_back(e):
        done = scatter_last(e)
        gathered = jnp.concatenate(
            [
                jnp.concatenate(
                    [
                        done[slot * n_ep : (slot + 1) * n_ep, c * part_w : (c + 1) * part_w]
                        for slot in range(CAPS)
                    ],
                    axis=1,
                )
                for c in range(parts_n)
            ],
            axis=0,
        )
        back_slab[e] = mm(turn_back, gathered).astype(BF16).reshape(
            n_ep, parts_n, CAPS * part_w
        )
        exchange(back_slab, back, b_send, b_recv, e)
        back[e, ep] = back_slab[e, ep]

    weights_out(1)
    send_back(0)
    weights_in(1)
    run(project, 0, n_z // 2)
    send_back(1)
    mixer_out()
    code = [upright(code_row[k : k + 1, :]) for k in range(2)]
    share_of = [upright(rw_ref[k : k + 1, :]) for k in range(2)]
    code, share_of = (
        [jnp.concatenate([c] * parts_n, axis=0) for c in cs] for cs in (code, share_of)
    )
    shape = (parts_n * tokens, group)
    same_part = iota(shape, 1) % parts_n == iota(shape, 0) // tokens
    mixes = []
    for e in range(2):
        for slot in range(CAPS):
            key = (iota(shape, 1) // parts_n * 8 + 4 * e + slot).astype(F32)
            share = jnp.zeros(shape, F32)
            for k in range(2):
                share = share + jnp.where((code[k] == key) & same_part, share_of[k], 0.0)
            high = share.astype(BF16)
            mixes.append((high, (share - high.astype(F32)).astype(BF16)))

    once = [
        (arrived.at[0, 1:], a_send.at[0]),
        (arrived.at[1, 1:], a_send.at[1]),
        (loc_vg.at[:, :, : (n_z - 1) * unit], c_send.at[0]),
        (loc_o.at[:, : (n_z - 1) * o_unit, :], c_send.at[1]),
        (vg_all.at[:, :, 0, :, : 15 * unit], p_send.at[0]),
        (o_all.at[:, :, : 15 * o_unit, :128], p_send.at[1]),
        (vg_all.at[:, :, 0], t_send.at[0]),
        (o_all.at[:, :, :, :128], t_send.at[1]),
        (rows.at[:, : n_z - 1, 0], g_send.at[0]),
        (parts.at[:, : n_z - 1, 0], s_send.at[0]),
        (rows.at[:, :, 0], m_send.at[0]),
        (parts.at[:, :, 1], q_send.at[0]),
    ]
    for ref, sem in once:
        bulk(ref, sem, o_sem.at[1]).wait_send()
    rim_copy.wait_send()

    combined = jnp.zeros((parts_n * tokens, part_w), F32)
    for e in range(2):
        bulk(back.at[e, 1:], b_send.at[e], b_recv.at[e]).wait_recv()
        results = back[e].reshape(group, CAPS * part_w)
        for slot in range(CAPS):
            high, low = mixes[e * CAPS + slot]
            part = results[:, slot * part_w : (slot + 1) * part_w]
            combined = combined + mm(high, part) + mm(low, part)
    square = jnp.sum(combined * combined, axis=1, keepdims=True)
    square = sum(square[c * tokens : (c + 1) * tokens] for c in range(parts_n))
    scale = lax.rsqrt(square / width + RMS_EPSILON)
    for c in range(parts_n):
        cols = slice(c * part_w, (c + 1) * part_w)
        out_ref[:, cols] = (
            combined[c * tokens : (c + 1) * tokens] * scale * egain_ref[:, cols]
        ).astype(BF16)
    for e in range(2):
        bulk(back.at[e, 1:], b_send.at[e], b_recv.at[e]).wait_send()


def on_device(
    mixer_in,
    pre_gain,
    glu_value,
    glu_gate,
    conv_kernel,
    chan_gain,
    out_weight,
    mix_gain,
    expert_in,
    ffn_gain,
    routing,
    route_weight,
    gate_proj,
    up_proj,
    down_proj,
    expert_gain,
):
    n_ep, n_z = lax.axis_size("ep"), lax.axis_size("tp") // 2
    half_z = n_z // 2
    tokens, width = expert_in.shape
    length = mixer_in.shape[0]
    slab_w, cap, hid = CAPS * (width // 8), n_ep * CAPS, gate_proj.shape[2]
    channels, cols = conv_kernel.shape[1], glu_value.shape[1]
    wide = out_weight.shape[1]
    rim_size = 32
    dma = pltpu.SemaphoreType.DMA
    vmem = pl.BlockSpec(memory_space=pltpu.VMEM)
    hbm = pl.BlockSpec(memory_space=pl.ANY)
    routed, mixed = pl.pallas_call(
        functools.partial(both_kernel, n_ep, n_z),
        out_shape=(
            pltpu.VMEM((tokens, width), BF16),
            pltpu.VMEM((length, width), BF16),
        ),
        in_specs=[vmem] * 8 + [hbm] * 7,
        out_specs=(vmem, vmem),
        scratch_shapes=[
            pltpu.VMEM((2, width, hid), BF16),
            pltpu.VMEM((2, width, hid), BF16),
            pltpu.VMEM((2, hid, width), BF16),
            pltpu.VMEM((rim_size + length, width), BF16),
            pltpu.VMEM((2, cols, width), BF16),
            pltpu.VMEM((2, channels // 2, wide), BF16),
            pltpu.VMEM((2, n_ep, 8, slab_w), BF16),
            pltpu.VMEM((2, n_ep, 8, slab_w), BF16),
            pltpu.VMEM((2, n_z, 2, cap, width), BF16),
            pltpu.VMEM((2, n_z, 2, cap, width), BF16),
            pltpu.VMEM((2, n_z, cap, width), BF16),
            pltpu.VMEM((2, 2, half_z, cap, width), BF16),
            pltpu.VMEM((2, n_ep, 8, slab_w), BF16),
            pltpu.VMEM((2, n_ep, 8, slab_w), BF16),
            pltpu.VMEM((n_z, 2, 2, cols, width), BF16),
            pltpu.VMEM((2, n_z, channels // 2, 2 * wide), BF16),
            pltpu.VMEM((rim_size + length, width), BF16),
            pltpu.VMEM((n_z, rim_size + length, 2 * cols), F32),
            pltpu.VMEM((length, channels), F32),
            pltpu.VMEM((length, channels), BF16),
            pltpu.VMEM((length, width), F32),
            dma((7,)),
            dma((2,)),
            dma((2,)),
            dma((1,)),
            dma((2, 2, half_z)),
            dma((1,)),
            dma((2, n_z)),
            dma((1,)),
            dma((2, n_z)),
            dma((1,)),
            dma((2, 2, half_z + 1)),
            dma((2,)),
            dma((2,)),
            dma((2,)),
            dma((2,)),
            dma((2,)),
            dma((2, 2, 8)),
            dma((2,)),
            dma((2,)),
            dma((4,)),
            dma((2,)),
        ],
        compiler_params=pltpu.CompilerParams(
            collective_id=0, has_side_effects=True, vmem_limit_bytes=60 * 1024 * 1024
        ),
        name="both_modules",
    )(
        expert_in,
        ffn_gain.reshape(1, -1),
        routing.T,
        route_weight.T,
        expert_gain.reshape(1, -1),
        pre_gain.reshape(1, -1),
        conv_kernel,
        chan_gain.reshape(1, -1),
        gate_proj,
        up_proj,
        down_proj,
        mixer_in,
        glu_value.T,
        glu_gate.T,
        out_weight.reshape(2, channels // 2, wide),
    )
    return ((mixed.astype(F32) * mix_gain).astype(BF16), routed)


def solution(mesh):
    in_specs = (
        P(("ep", "tp"), None),
        P(),
        P(None, "tp"),
        P(None, "tp"),
        P(),
        P(),
        P(None, "tp"),
        P(),
        P(("ep", "tp"), None),
        P(),
        P(("ep", "tp"), None),
        P(("ep", "tp"), None),
        P("ep", None, "tp"),
        P("ep", None, "tp"),
        P("ep", "tp", None),
        P(),
    )
    out_specs = (P(("ep", "tp"), None), P(("ep", "tp"), None))
    return jax.shard_map(
        on_device, mesh=mesh, in_specs=in_specs, out_specs=out_specs, check_vma=False
    )
```

```python
import functools

import jax
import jax.numpy as jnp
from jax import lax
from jax.experimental import pallas as pl
from jax.experimental.pallas import tpu as pltpu
from jax.sharding import PartitionSpec as P

RMS_EPSILON = 1e-06
LAYER_EPSILON = 1e-05
CLAMP_LIMIT = 7.0
SWISH_ALPHA = 1.702
CAPS = 3
MESH = pl.DeviceIdType.MESH
F32 = jnp.float32
BF16 = jnp.bfloat16


def iota(shape, dim):
    return lax.broadcasted_iota(jnp.int32, shape, dim)


def mm(a, b):
    return jnp.dot(a, b, preferred_element_type=F32)


def rms_scale(values, gain_row):
    values = values.astype(F32)
    return (
        values
        * lax.rsqrt(jnp.mean(values * values, axis=-1, keepdims=True) + RMS_EPSILON)
        * gain_row
    )


def both_kernel(
    n_ep,
    n_z,
    x_ref,
    fgain_ref,
    route_ref,
    rw_ref,
    egain_ref,
    pgain_ref,
    taps_ref,
    cgain_ref,
    mgain_ref,
    gate_hbm,
    up_hbm,
    down_hbm,
    mix_hbm,
    value_hbm,
    glu_hbm,
    ow_hbm,
    out_ref,
    mixed_ref,
    gate_v,
    up_v,
    down_v,
    mix_v,
    loc_vg,
    loc_o,
    slab,
    arrived,
    rows,
    parts,
    mate,
    ring_in,
    back_slab,
    back,
    vg_all,
    o_all,
    normed_v,
    ext,
    conv_v,
    act_v,
    proj_v,
    w_sem,
    a_send,
    a_recv,
    g_send,
    g_recv,
    m_send,
    m_recv,
    q_send,
    q_recv,
    s_send,
    s_recv,
    b_send,
    b_recv,
    c_send,
    c_recv,
    p_send,
    p_recv,
    t_send,
    t_recv,
    h_sem,
    o_sem,
):
    half_z = n_z // 2
    n_s = 4
    tokens, width = x_ref.shape
    cap = n_ep * CAPS
    slots = n_ep * 16
    parts_n = 8
    part_w = width // parts_n
    length = mix_hbm.shape[0]
    rim_size = mix_v.shape[0] - length
    unit = width // n_ep
    o_unit = loc_o.shape[1] // n_ep
    ep, tp = lax.axis_index("ep"), lax.axis_index("tp")
    z, core = tp // 2, tp % 2
    mate_tp = 2 * z + 1 - core
    next_tp = 2 * ((z + 1) % n_z) + core
    prev_tp = 2 * ((z + n_z - 1) % n_z) + core
    toward = {1: next_tp, -1: prev_tp}
    side = {1: 0, -1: 1}
    major = (ep // n_s, ep % n_s)
    minor = (ep % n_s, ep // n_s)
    after = (tp + 1) // (2 * n_z)
    line_next = ((ep + after) % n_ep, (tp + 1) % (2 * n_z))
    behind = (2 * n_z - tp) // (2 * n_z)
    line_prev = ((ep + n_ep - behind) % n_ep, (tp + 2 * n_z - 1) % (2 * n_z))

    def pos(d):
        return 2 * d - 1 if d > 0 else -2 * d

    def place(d):
        return n_z - 1 if d in (half_z, -half_z) else pos(d)

    def cols_of(way, k):
        if k < half_z:
            return slice(0, width)
        return pl.ds(side[way] * (width // 2), width // 2)

    def send(src, dst, send_sem, recv_sem, device):
        return pltpu.make_async_remote_copy(
            src_ref=src,
            dst_ref=dst,
            send_sem=send_sem,
            recv_sem=recv_sem,
            device_id=device,
            device_id_type=MESH,
        )

    def bulk(ref, send_sem, recv_sem):
        return send(ref, ref, send_sem, recv_sem, (ep, mate_tp))

    def run(fn, low, high, unroll=1):
        def body(i, carry):
            fn(i)
            return carry

        lax.fori_loop(low, high, body, 0, unroll=unroll)

    def lanes(i, n):
        return pl.ds(pl.multiple_of(i * n, n), n)

    loads = [
        pltpu.make_async_copy(src, dst, w_sem.at[i])
        for i, (src, dst) in enumerate(
            (
                (value_hbm, loc_vg.at[0]),
                (glu_hbm, loc_vg.at[1]),
                (ow_hbm, loc_o),
                (gate_hbm, gate_v),
                (up_hbm, up_v),
                (down_hbm, down_v),
                (mix_hbm, mix_v.at[rim_size:]),
            )
        )
    ]
    for load in loads:
        load.start()

    barrier = pltpu.get_barrier_semaphore()

    def greet(device):
        pl.semaphore_signal(barrier, inc=1, device_id=device, device_id_type=MESH)

    run(lambda i: greet(((ep + i) % n_ep, tp)), 1, n_ep)
    run(lambda i: greet((ep, 2 * ((z + i) % n_z) + core)), 1, n_z)
    for device in ((ep, mate_tp), line_next, line_prev):
        greet(device)

    experts = 2 * n_ep
    eye = iota((tokens, tokens), 0) == iota((tokens, tokens), 1)

    def upright(row):
        return jnp.sum(jnp.where(eye, row, 0.0), axis=1, keepdims=True)

    chosen = [route_ref[k : k + 1, :] for k in range(2)]
    named = [(c == iota((experts, tokens), 0)).astype(F32) for c in chosen]
    earlier = (iota((tokens, tokens), 0) < iota((tokens, tokens), 1)).astype(F32)
    before = mm((named[0] + named[1]).astype(BF16), earlier.astype(BF16))
    code_row = jnp.concatenate(
        [
            c.astype(F32) * 4.0 + jnp.sum(before * n, axis=0, keepdims=True)
            for c, n in zip(chosen, named)
        ],
        axis=0,
    )
    spread = (iota((tokens, parts_n * tokens), 1) % tokens) == iota(
        (tokens, parts_n * tokens), 0
    )
    code_wide = mm(code_row.astype(BF16), spread.astype(F32).astype(BF16))
    normed = rms_scale(x_ref[...], fgain_ref[...]).astype(BF16)
    stacked = jnp.concatenate(
        [normed[:, c * part_w : (c + 1) * part_w] for c in range(parts_n)], axis=0
    )
    group = n_ep * parts_n
    shape = (group, parts_n * tokens)
    same_part = iota(shape, 0) % parts_n == iota(shape, 1) // tokens
    for e in range(2):
        for slot in range(CAPS):
            key = (iota(shape, 0) // parts_n * 8 + 4 * e + slot).astype(F32)
            hit = (code_wide[0:1] == key) | (code_wide[1:2] == key)
            picked = mm(jnp.where(hit & same_part, 1.0, 0.0).astype(BF16), stacked)
            slab[e, :, :, slot * part_w : (slot + 1) * part_w] = picked.astype(
                BF16
            ).reshape(n_ep, parts_n, part_w)
    pl.semaphore_wait(barrier, n_ep - 1 + n_z - 1 + 3)

    offsets = sorted(
        [(dy, dx) for dy in range(n_s) for dx in range(n_s) if dy or dx],
        key=lambda d: -(min(d[0], n_s - d[0]) + min(d[1], n_s - d[1])),
    )

    def exchange(src, dst, send_sem, recv_sem, e):
        for dy, dx in offsets:
            peer = ((ep // n_s + dy) % n_s) * n_s + (ep % n_s + dx) % n_s
            send(
                src.at[e, peer], dst.at[e, ep], send_sem.at[e], recv_sem.at[e], (peer, tp)
            ).start()

    rim_copy = send(
        mix_hbm.at[length - rim_size :],
        mix_v.at[:rim_size],
        o_sem.at[0],
        o_sem.at[1],
        line_next,
    )
    for e in range(2):
        exchange(slab, arrived, a_send, a_recv, e)

    piece = [major[i] * n_s + minor[i] for i in range(2)]

    def vg_at(i, zs, who, at, count):
        return vg_all.at[zs, i, who, :, pl.ds(pl.multiple_of(at * unit, unit), count * unit)]

    def o_at(i, zs, who, at, count):
        return o_all.at[
            i, zs, pl.ds(pl.multiple_of(at * o_unit, o_unit), count * o_unit), lanes(who, 128)
        ]

    def piece_from(i, n):
        if n == 0:
            return loc_vg.at[i, :, lanes(piece[i], unit)]
        return loc_o.at[i, lanes(piece[i], o_unit), :]

    def region(i, zs, at, count, n):
        return vg_at(i, zs, core, at, count) if n == 0 else o_at(i, zs, core, at, count)

    def own_copy(i, n):
        return pltpu.make_async_copy(
            piece_from(i, n), region(i, z, piece[i], 1, n), h_sem.at[2 * i + n]
        )

    def column_send(n):
        def one(dz):
            for i in range(2):
                send(
                    piece_from(i, n),
                    region(i, z, piece[i], 1, n),
                    c_send.at[n],
                    c_recv.at[n],
                    (ep, 2 * ((z + dz) % n_z) + core),
                ).start()

        run(one, 1, n_z)
        for i in range(2):
            own_copy(i, n).start()

    for load in loads[:2]:
        load.wait()
    column_send(0)
    rim_copy.start()
    for e in range(2):
        arrived[e, ep] = slab[e, ep]

    def plane(i, phase, way, step, n):
        a, b = major[i], minor[i]
        zs = pl.ds(0, n_z) if step == 0 else pl.ds(0 if way == 1 else half_z, half_z)
        if phase == 0:
            source = (b + n_s - way * step) % n_s
            at, count = a * n_s + source, 1
            there = (a, (b + n_s + way) % n_s)
        else:
            source = (a + n_s - way * step) % n_s
            at, count = source * n_s, n_s
            there = ((a + n_s + way) % n_s, b)
        ref = region(i, zs, at, count, n)
        return send(
            ref,
            ref,
            p_send.at[n],
            p_recv.at[i, phase, 2 * (2 * step + side[way]) + n],
            (there[0] * n_s + there[1] if i == 0 else there[1] * n_s + there[0], tp),
        )

    def plane_mate(i, turn, n):
        shift = (0, n_s - 1, 1, 2)[turn]
        at = ((major[i] + shift) % n_s) * n_s
        ref = region(i, pl.ds(0, n_z), at, n_s, n)
        return send(ref, ref, t_send.at[n], t_recv.at[n], (ep, mate_tp))


    def turned(across):
        turn = iota((group, group), 1 - across)
        hit = iota((group, group), across) == turn % n_ep * parts_n + turn // n_ep
        return jnp.where(hit, 1.0, 0.0).astype(BF16)

    def ring(way, e, k):
        cols = cols_of(way, k)
        return send(
            rows.at[e, place(-way * (k - 1)), 0, :, cols],
            rows.at[e, place(-way * k), 0, :, cols],
            g_send.at[0],
            g_recv.at[side[way], e, k - 1],
            (ep, toward[way]),
        )

    def to_mate(e, p):
        return send(
            rows.at[e, p, 0], rows.at[e, p, 1], m_send.at[0], m_recv.at[e, p], (ep, mate_tp)
        )

    def part_to_mate(e, p):
        return send(
            parts.at[e, p, 1], mate.at[e, p], q_send.at[0], q_recv.at[e, p], (ep, mate_tp)
        )

    def ring_sum(way, e, k, early=False):
        cols, mark = cols_of(way, k), k - 1
        if k == half_z - 1:
            cols = cols_of(-way if early else way, half_z)
            mark = half_z if early else mark
        return send(
            parts.at[e, place(way * k), 0, :, cols],
            ring_in.at[side[way], e, k - 1, :, cols],
            s_send.at[0],
            s_recv.at[side[way], e, mark],
            (ep, toward[way]),
        )

    turn_in = turned(1)

    def take_in(e):
        bulk(arrived.at[e, 1:], a_send.at[e], a_recv.at[e]).wait_recv()
        block = mm(turn_in, arrived[e].reshape(group, CAPS * part_w)).astype(BF16)
        for c in range(parts_n):
            at = c * n_ep
            for slot in range(CAPS):
                rows[
                    e, 0, 0, slot * n_ep : (slot + 1) * n_ep, c * part_w : (c + 1) * part_w
                ] = block[at : at + n_ep, slot * part_w : (slot + 1) * part_w]
        if e == 0:
            for way in (1, -1):
                ring(way, e, 1).start()
        to_mate(e, 0).start()

    take_in(0)
    take_in(1)

    column_bulk = [
        bulk(loc_vg.at[:, :, : (n_z - 1) * unit], c_send.at[0], c_recv.at[0]),
        bulk(loc_o.at[:, : (n_z - 1) * o_unit, :], c_send.at[1], c_recv.at[1]),
    ]

    def columns_in(n):
        column_bulk[n].wait_recv()
        for i in range(2):
            own_copy(i, n).wait()
        for i in range(2):
            for way in (1, -1):
                plane(i, 0, way, 0, n).start()

    for load in loads[2:]:
        load.wait()

    def ffn(e, low, high):
        for p in range(low, high):
            to_mate(e, p).wait_recv()
        count = (high - low) * 2 * cap
        block = rows[e, low:high].reshape(count, width)
        gate = jnp.minimum(mm(block, gate_v[e]), CLAMP_LIMIT)
        up = jnp.clip(mm(block, up_v[e]), -CLAMP_LIMIT, CLAMP_LIMIT)
        hidden = ((up + 1.0) * gate * jax.nn.sigmoid(SWISH_ALPHA * gate)).astype(BF16)
        parts[e, low:high] = (
            mm(hidden, down_v[e]).astype(BF16).reshape(high - low, 2, cap, width)
        )
        for p in range(low, high):
            part_to_mate(e, p).start()

    def chip_sum(e, low, high):
        for p in range(low, high):
            part_to_mate(e, p).wait_recv()

        def add(p):
            parts[e, p, 0] = (
                parts[e, p, 0].astype(F32) + mate[e, p].astype(F32)
            ).astype(BF16)

        run(add, low, high)

    def plane_forward(phase, n):
        for i in range(2):
            for way in (1, -1):
                plane(i, phase, way, 0, n).wait_recv()
                plane(i, phase, way, 1, n).start()

    def phase_two(n):
        for i in range(2):
            for way in (1, -1):
                plane(i, 0, way, 1, n).wait_recv()
            for way in (1, -1):
                plane(i, 1, way, 0, n).start()
            plane_mate(i, 0, n).start()

    def weights_out(n):
        for i in range(2):
            for way in (1, -1):
                plane(i, 1, way, 1, n).wait_recv()
            plane_mate(i, 3, n).start()

    def weights_mid(n):
        for i in range(2):
            for turn in (1, 2):
                plane_mate(i, turn, n).start()

    def gather_step(e, k, way):
        ring(way, e, k).wait_recv()
        if k < half_z:
            ring(way, e, k + 1).start()
            to_mate(e, place(-way * k)).start()

    def gather_far(e):
        for way in (1, -1):
            gather_step(e, half_z, way)
        to_mate(e, place(half_z)).start()

    def scatter_first(e):
        for way in (1, -1):
            ring_sum(way, e, half_z).start()

    def scatter_early(e):
        for way in (1, -1):
            ring_sum(way, e, half_z - 1, True).start()

    def scatter_step(e, k, way):
        ring_sum(way, e, k + 1).wait_recv()
        if k == half_z - 2:
            ring_sum(way, e, k + 1, True).wait_recv()
        p, cols = place(way * k), cols_of(way, k + 1)
        parts[e, p, 0, :, cols] = (
            parts[e, p, 0, :, cols].astype(F32)
            + ring_in[side[way], e, k, :, cols].astype(F32)
        ).astype(BF16)
        ring_sum(way, e, k).start()

    def scatter_last(e):
        total = parts[e, 0, 0].astype(F32)
        for way in (1, -1):
            ring_sum(way, e, 1).wait_recv()
            total = total + ring_in[side[way], e, 0].astype(F32)
        return total.astype(BF16)

    def norm_mix(i):
        at = pl.ds(pl.multiple_of(i * 16, 16), 16)
        normed_v[at, :] = rms_scale(mix_v[at, :], pgain_ref[...]).astype(BF16)

    def nt(a, b):
        return lax.dot_general(a, b, (((1,), (1,)), ((), ())), preferred_element_type=F32)

    def glu(i):
        a = normed_v[...]
        pre = nt(a, vg_all[i].reshape(256, width))
        gated = (pre[:, :128] * jax.nn.sigmoid(pre[:, 128:])).astype(BF16).astype(F32)
        ext[i] = jnp.where(real, gated, 0.0)

    taps = taps_ref.shape[0]
    lead = rim_size - (taps - 1)
    blocks = 2
    span = length // blocks
    real = iota((rim_size + length, 128), 0) >= jnp.where((ep + tp) == 0, rim_size, 0)

    def conv(n):
        i, at = n // blocks, (n % blocks) * span
        acc = jnp.zeros((span, 128), F32)
        for r in range(8):
            picks = [j for j in range(taps) if (j + lead) % 8 == r]
            reach = max((j + lead) // 8 for j in picks) * 8
            moved = ext[i, pl.ds(at + r, span + reach), :]
            for j in picks:
                q = (j + lead) // 8 * 8
                acc = acc + taps_ref[j : j + 1, lanes(i, 128)] * moved[q : q + span]
        conv_v[pl.ds(pl.multiple_of(at, 8), span), lanes(i, 128)] = acc

    def activate(i):
        at = pl.ds(pl.multiple_of(i * 32, 32), 32)
        c = conv_v[at, :]
        c = c - jnp.mean(c, axis=-1, keepdims=True)
        var = jnp.mean(c * c, axis=-1, keepdims=True)
        c = c * lax.rsqrt(var + LAYER_EPSILON) * cgain_ref[...]
        act_v[at, :] = (c * jax.nn.sigmoid(c)).astype(BF16)

    def project(i):
        mid = act_v.shape[1] // 2
        proj_v[:, lanes(i, 256)] = mm(act_v[:, :mid], o_all[0, i]) + mm(
            act_v[:, mid:], o_all[1, i]
        )

    def norm_out(i):
        at = pl.ds(pl.multiple_of(i * 16, 16), 16)
        mixed_ref[at, :] = rms_scale(proj_v[at, :], mgain_ref[...]).astype(BF16)

    def weights_in(n):
        ref = (vg_all.at[:, :, 0], o_all.at[:, :, :, :128])[n]
        bulk(ref, t_send.at[n], t_recv.at[n]).wait_recv()

    def mixer_glu(low, high):
        run(glu, low, high)

    def mixer_conv(low, high):
        run(conv, low, high)

    def mixer_act():
        run(activate, 0, length // 32, 2)

    def norm_mix_all():
        rim_copy.wait_recv()
        run(norm_mix, 0, (rim_size + length) // 16, 2)

    def mixer_out():
        run(project, n_z // 2, n_z)
        run(norm_out, 0, length // 16, 2)

    ffn(0, 0, 1)
    columns_in(0)
    norm_mix_all()
    for way in (1, -1):
        ring(way, 1, 1).start()
    gather_step(0, 1, -1)
    gather_step(0, 1, 1)
    ffn(1, 0, 1)
    plane_forward(0, 0)
    gather_step(1, 1, 1)
    gather_step(1, 1, -1)
    gather_step(0, 2, -1)
    gather_step(0, 2, 1)
    phase_two(0)
    ffn(0, 1, 3)
    gather_step(1, 2, -1)
    gather_step(1, 2, 1)
    ffn(1, 1, 3)
    chip_sum(0, 0, 3)
    gather_step(0, 3, 1)
    gather_step(0, 3, -1)
    ffn(0, 3, 5)
    chip_sum(1, 0, 3)
    ffn(1, 3, 5)
    gather_step(1, 3, -1)
    gather_step(1, 3, 1)
    column_send(1)
    ffn(0, 5, 7)
    ffn(1, 5, 7)
    gather_far(0)
    chip_sum(0, 5, 7)
    scatter_early(0)
    plane_forward(1, 0)
    chip_sum(0, 3, 5)
    chip_sum(1, 3, 5)
    ffn(0, 7, 8)
    gather_far(1)
    chip_sum(1, 5, 7)
    chip_sum(0, 7, 8)
    scatter_first(0)
    scatter_early(1)
    ffn(1, 7, 8)
    chip_sum(1, 7, 8)
    scatter_first(1)
    weights_mid(0)
    columns_in(1)

    scatter_step(0, 3, 1)
    scatter_step(0, 3, -1)
    plane_forward(0, 1)
    scatter_step(1, 3, -1)
    scatter_step(1, 3, 1)
    weights_out(0)
    phase_two(1)
    scatter_step(0, 2, -1)
    scatter_step(0, 2, 1)
    weights_in(0)
    mixer_glu(0, 4)
    scatter_step(1, 2, -1)
    scatter_step(1, 2, 1)
    mixer_glu(4, n_z)
    mixer_conv(0, n_z * blocks)
    scatter_step(0, 1, 1)
    scatter_step(0, 1, -1)
    plane_forward(1, 1)
    weights_mid(1)
    mixer_act()
    scatter_step(1, 1, 1)
    scatter_step(1, 1, -1)

    turn_back = turned(0)

    def send_back(e):
        done = scatter_last(e)
        gathered = jnp.concatenate(
            [
                jnp.concatenate(
                    [
                        done[slot * n_ep : (slot + 1) * n_ep, c * part_w : (c + 1) * part_w]
                        for slot in range(CAPS)
                    ],
                    axis=1,
                )
                for c in range(parts_n)
            ],
            axis=0,
        )
        back_slab[e] = mm(turn_back, gathered).astype(BF16).reshape(
            n_ep, parts_n, CAPS * part_w
        )
        exchange(back_slab, back, b_send, b_recv, e)
        back[e, ep] = back_slab[e, ep]

    weights_out(1)
    send_back(0)
    weights_in(1)
    run(project, 0, n_z // 2)
    send_back(1)
    mixer_out()
    code = [upright(code_row[k : k + 1, :]) for k in range(2)]
    share_of = [upright(rw_ref[k : k + 1, :]) for k in range(2)]
    code, share_of = (
        [jnp.concatenate([c] * parts_n, axis=0) for c in cs] for cs in (code, share_of)
    )
    shape = (parts_n * tokens, group)
    same_part = iota(shape, 1) % parts_n == iota(shape, 0) // tokens
    mixes = []
    for e in range(2):
        for slot in range(CAPS):
            key = (iota(shape, 1) // parts_n * 8 + 4 * e + slot).astype(F32)
            share = jnp.zeros(shape, F32)
            for k in range(2):
                share = share + jnp.where((code[k] == key) & same_part, share_of[k], 0.0)
            high = share.astype(BF16)
            mixes.append((high, (share - high.astype(F32)).astype(BF16)))

    once = [
        (arrived.at[0, 1:], a_send.at[0]),
        (arrived.at[1, 1:], a_send.at[1]),
        (loc_vg.at[:, :, : (n_z - 1) * unit], c_send.at[0]),
        (loc_o.at[:, : (n_z - 1) * o_unit, :], c_send.at[1]),
        (vg_all.at[:, :, 0, :, : 15 * unit], p_send.at[0]),
        (o_all.at[:, :, : 15 * o_unit, :128], p_send.at[1]),
        (vg_all.at[:, :, 0], t_send.at[0]),
        (o_all.at[:, :, :, :128], t_send.at[1]),
        (rows.at[:, : n_z - 1, 0], g_send.at[0]),
        (parts.at[:, : n_z - 1, 0], s_send.at[0]),
        (rows.at[:, :, 0], m_send.at[0]),
        (parts.at[:, :, 1], q_send.at[0]),
    ]
    for ref, sem in once:
        bulk(ref, sem, o_sem.at[1]).wait_send()
    rim_copy.wait_send()

    combined = jnp.zeros((parts_n * tokens, part_w), F32)
    for e in range(2):
        bulk(back.at[e, 1:], b_send.at[e], b_recv.at[e]).wait_recv()
        results = back[e].reshape(group, CAPS * part_w)
        for slot in range(CAPS):
            high, low = mixes[e * CAPS + slot]
            part = results[:, slot * part_w : (slot + 1) * part_w]
            combined = combined + mm(high, part) + mm(low, part)
    square = jnp.sum(combined * combined, axis=1, keepdims=True)
    square = sum(square[c * tokens : (c + 1) * tokens] for c in range(parts_n))
    scale = lax.rsqrt(square / width + RMS_EPSILON)
    for c in range(parts_n):
        cols = slice(c * part_w, (c + 1) * part_w)
        out_ref[:, cols] = (
            combined[c * tokens : (c + 1) * tokens] * scale * egain_ref[:, cols]
        ).astype(BF16)
    for e in range(2):
        bulk(back.at[e, 1:], b_send.at[e], b_recv.at[e]).wait_send()


def write_results(mixed_ref, routed_ref, mixed_hbm, routed_hbm, sem):
    rows = mixed_ref.shape[0] // 4
    copies = [pltpu.make_async_copy(routed_ref, routed_hbm, sem.at[4])]
    for i in range(4):
        at = slice(i * rows, (i + 1) * rows)
        copies.append(
            pltpu.make_async_copy(mixed_ref.at[at, :], mixed_hbm.at[at, :], sem.at[i])
        )
    for copy in copies:
        copy.start()
    for copy in copies:
        copy.wait()


def on_device(
    mixer_in,
    pre_gain,
    glu_value,
    glu_gate,
    conv_kernel,
    chan_gain,
    out_weight,
    mix_gain,
    expert_in,
    ffn_gain,
    routing,
    route_weight,
    gate_proj,
    up_proj,
    down_proj,
    expert_gain,
):
    n_ep, n_z = lax.axis_size("ep"), lax.axis_size("tp") // 2
    half_z = n_z // 2
    tokens, width = expert_in.shape
    length = mixer_in.shape[0]
    slab_w, cap, hid = CAPS * (width // 8), n_ep * CAPS, gate_proj.shape[2]
    channels, cols = conv_kernel.shape[1], glu_value.shape[1]
    wide = out_weight.shape[1]
    rim_size = 32
    dma = pltpu.SemaphoreType.DMA
    vmem = pl.BlockSpec(memory_space=pltpu.VMEM)
    hbm = pl.BlockSpec(memory_space=pl.ANY)
    routed, mixed = pl.pallas_call(
        functools.partial(both_kernel, n_ep, n_z),
        out_shape=(
            pltpu.VMEM((tokens, width), BF16),
            pltpu.VMEM((length, width), BF16),
        ),
        in_specs=[vmem] * 9 + [hbm] * 7,
        out_specs=(vmem, vmem),
        scratch_shapes=[
            pltpu.VMEM((2, width, hid), BF16),
            pltpu.VMEM((2, width, hid), BF16),
            pltpu.VMEM((2, hid, width), BF16),
            pltpu.VMEM((rim_size + length, width), BF16),
            pltpu.VMEM((2, cols, width), BF16),
            pltpu.VMEM((2, channels // 2, wide), BF16),
            pltpu.VMEM((2, n_ep, 8, slab_w), BF16),
            pltpu.VMEM((2, n_ep, 8, slab_w), BF16),
            pltpu.VMEM((2, n_z, 2, cap, width), BF16),
            pltpu.VMEM((2, n_z, 2, cap, width), BF16),
            pltpu.VMEM((2, n_z, cap, width), BF16),
            pltpu.VMEM((2, 2, half_z, cap, width), BF16),
            pltpu.VMEM((2, n_ep, 8, slab_w), BF16),
            pltpu.VMEM((2, n_ep, 8, slab_w), BF16),
            pltpu.VMEM((n_z, 2, 2, cols, width), BF16),
            pltpu.VMEM((2, n_z, channels // 2, 2 * wide), BF16),
            pltpu.VMEM((rim_size + length, width), BF16),
            pltpu.VMEM((n_z, rim_size + length, 2 * cols), F32),
            pltpu.VMEM((length, channels), F32),
            pltpu.VMEM((length, channels), BF16),
            pltpu.VMEM((length, width), F32),
            dma((7,)),
            dma((2,)),
            dma((2,)),
            dma((1,)),
            dma((2, 2, half_z)),
            dma((1,)),
            dma((2, n_z)),
            dma((1,)),
            dma((2, n_z)),
            dma((1,)),
            dma((2, 2, half_z + 1)),
            dma((2,)),
            dma((2,)),
            dma((2,)),
            dma((2,)),
            dma((2,)),
            dma((2, 2, 8)),
            dma((2,)),
            dma((2,)),
            dma((4,)),
            dma((2,)),
        ],
        compiler_params=pltpu.CompilerParams(
            collective_id=0, has_side_effects=True, vmem_limit_bytes=60 * 1024 * 1024
        ),
        name="both_modules",
    )(
        expert_in,
        ffn_gain.reshape(1, -1),
        routing.T,
        route_weight.T,
        expert_gain.reshape(1, -1),
        pre_gain.reshape(1, -1),
        conv_kernel,
        chan_gain.reshape(1, -1),
        mix_gain.reshape(1, -1),
        gate_proj,
        up_proj,
        down_proj,
        mixer_in,
        glu_value.T,
        glu_gate.T,
        out_weight.reshape(2, channels // 2, wide),
    )
    return pl.pallas_call(
        write_results,
        out_shape=(
            jax.ShapeDtypeStruct((length, width), BF16),
            jax.ShapeDtypeStruct((tokens, width), BF16),
        ),
        in_specs=[vmem] * 2,
        out_specs=(hbm, hbm),
        scratch_shapes=[dma((5,))],
        compiler_params=pltpu.CompilerParams(vmem_limit_bytes=4 * 1024 * 1024),
        name="write_results",
    )(mixed, routed)


def solution(mesh):
    in_specs = (
        P(("ep", "tp"), None),
        P(),
        P(None, "tp"),
        P(None, "tp"),
        P(),
        P(),
        P(None, "tp"),
        P(),
        P(("ep", "tp"), None),
        P(),
        P(("ep", "tp"), None),
        P(("ep", "tp"), None),
        P("ep", None, "tp"),
        P("ep", None, "tp"),
        P("ep", "tp", None),
        P(),
    )
    out_specs = (P(("ep", "tp"), None), P(("ep", "tp"), None))
    return jax.shard_map(
        on_device, mesh=mesh, in_specs=in_specs, out_specs=out_specs, check_vma=False
    )
```
